256 devices in a mesh: sp: 128 (over z, y, x), tp: 2 (over core).
Axes of the slice: x: 4, y: 4, z: 8, core: 2. Of those that a mesh axis runs over, the one named last changes fastest.
Arguments:
- conv_value: bfloat16 [65536, 1536], P('sp', 'tp'), may hold values from -6 to 6
- conv_gate: bfloat16 [65536, 1536], P('sp', 'tp'), may hold values from -8 to 8
- conv_out: bfloat16 [65536, 1536], P('sp', 'tp'), may hold values from -40 to 40
- conv_taps: bfloat16 [31, 1536], P(None, 'tp'), may hold values from -1 to 1
- norm_gain: float32 [1536], P('tp'), may hold values from 0.1 to 1.9
- norm_shift: float32 [1536], P('tp'), may hold values from -3 to 3
- proj_weight: bfloat16 [2048, 1536], P(None, 'tp'), may hold values from -0.15625 to 0.15625
- out_grad: bfloat16 [65536, 2048], P('sp'), may hold values from -24 to 24
Outputs:
- grad_value: bfloat16 [65536, 1536], P('sp', 'tp')
- grad_gate: bfloat16 [65536, 1536], P('sp', 'tp')
- grad_taps: float32 [31, 1536], P(None, 'tp')
- grad_gain: float32 [1536], P('tp')
- grad_shift: float32 [1536], P('tp')
- grad_proj: float32 [2048, 1536], P('sp', 'tp')
The draws below stay inside these ranges and needn't reach their ends.
All inputs are finite; a program needn't handle non-finite values.
Results may differ from the reference program's by a relative error of at most 0.005.
Values may be sent and summed in bfloat16 or wider, within the bound.
No kernel may reach another device: no remote copies, remote signals or barrier semaphores. Data moves between devices by JAX's collectives and lax.ppermute only.
A program may use at most 64 MiB of HBM per device.

```python
import jax
import jax.numpy as jnp
from jax import lax

D = 2048
CH = 1536
TAPS = 31
SEQ = 65536


def draw_conv_out(key, part):
    key_scale, key_group, key_base, key_mean = jax.random.split(key, 4)
    chan_scale = jnp.exp(jax.random.uniform(key_scale, (CH,), jnp.float32, -1.0, 1.0))
    group_scale = jnp.exp(jax.random.uniform(key_group, (8,), jnp.float32, -1.2, 1.2))
    group_index = jnp.arange(CH) * 8 // CH
    scales = chan_scale * group_scale[group_index]
    base = jax.random.normal(key_base, (SEQ, CH), jnp.float32) * scales
    offset = jax.random.normal(key_mean, (SEQ, 1), jnp.float32)
    return jnp.clip(base + offset, -40.0, 40.0).astype(jnp.bfloat16)


def spiked(values, rng, source, target, parts, factor):
    def block_of(position):
        return (jnp.arange(values.shape[position]) // (values.shape[position] // parts)).reshape((-1,) + (1,) * (values.ndim - 1 - position))

    one_side = jax.random.permutation(rng, parts)[block_of(target)]
    other_side = (block_of(target) + parts // 2) % parts
    return jnp.where((block_of(source) == one_side) | (block_of(source) == other_side), factor * values, values)


def steps_of(stream_key, extent, shards, smallest, high):
    def one(axis_at, parts):
        steps = jax.random.uniform(jax.random.fold_in(jax.random.fold_in(stream_key, 6), axis_at), (parts,), jnp.float32, smallest / len(shards), high / len(shards))
        return jnp.repeat(jnp.exp(steps), extent[axis_at] // parts).reshape((-1,) + (1,) * (len(extent) - axis_at - 1))

    factor_of = one(*shards[0])
    for cut in shards[1:]:
        factor_of = factor_of * one(*cut)
    return factor_of


def bell_draw(own_key, dims, scale, limit, cuts=(), held_as=jnp.bfloat16):
    entries = jax.random.normal(own_key, dims, jnp.float32) * scale
    if len(cuts) > 0:
        entries = steps_of(own_key, dims, cuts, -0.22, 0.18) * entries
    return jnp.clip(entries, min=-limit, max=limit).astype(held_as)


def noise_with(key, extent, spread, reach, pieces, heavy, held_as=jnp.bfloat16):
    drawn = spread * jax.random.normal(key, extent, jnp.float32)
    if pieces:
        drawn = drawn * steps_of(key, extent, pieces, -0.22, 0.18)
    return jnp.clip(spiked(drawn, jax.random.fold_in(key, 3), *heavy), -reach, reach).astype(held_as)


def setup_inputs(seed: int = 0) -> dict:
    splits = jax.random.split(jax.random.key(seed), 9)
    return {
        "conv_value": bell_draw(splits[0], (SEQ, CH), 1.0, 6.0, ((0, 128), (1, 2))),
        "conv_gate": bell_draw(splits[1], (SEQ, CH), 1.5, 8.0, ((0, 128), (1, 2))),
        "conv_out": draw_conv_out(jax.random.fold_in(splits[8], 71), 0),
        "conv_taps": bell_draw(splits[3], (TAPS, CH), TAPS ** -0.5, 1.0, ((1, 2),)),
        "norm_gain": jnp.clip(1.0 + 0.18 * jax.random.normal(splits[4], (CH,), jnp.float32), 0.1, 1.9),
        "norm_shift": bell_draw(splits[5], (CH,), 0.5, 3.0, ((0, 2),), jnp.float32),
        "proj_weight": bell_draw(splits[6], (D, CH), CH ** -0.5, 0.15625, ((1, 2),)),
        "out_grad": noise_with(splits[7], (SEQ, D), 1.0, 24.0, ((0, 128),), (0, 1, 128, 5.5)),
    }


norm_eps = 1e-05

def reference(conv_value, conv_gate, conv_out, conv_taps, norm_gain, norm_shift, proj_weight, out_grad):
    height = conv_out.astype(jnp.float32)
    center = lax.optimization_barrier(jnp.mean(height, axis=1, keepdims=True))
    centered = height - center
    variance = lax.optimization_barrier(jnp.mean(centered * centered, axis=1, keepdims=True))
    inv_std = lax.rsqrt(variance + norm_eps)
    normed = centered * inv_std
    shifted = normed * norm_gain + norm_shift
    sig_norm = jax.nn.sigmoid(shifted)
    active = (shifted * sig_norm).astype(jnp.bfloat16)
    grad_proj = jnp.dot(out_grad.T, active, preferred_element_type=jnp.float32)
    act_grad = jnp.dot(out_grad, proj_weight, preferred_element_type=jnp.float32)
    norm_grad = act_grad * (sig_norm * (1.0 + shifted * (1.0 - sig_norm)))
    grad_gain = lax.optimization_barrier(jnp.sum(norm_grad * normed, axis=0))
    grad_shift = lax.optimization_barrier(jnp.sum(norm_grad, axis=0))
    scaled = norm_grad * norm_gain
    height_grad = inv_std * (scaled - lax.optimization_barrier(jnp.mean(scaled, axis=1, keepdims=True)) - normed * lax.optimization_barrier(jnp.mean(scaled * normed, axis=1, keepdims=True)))
    sig_gate = jax.nn.sigmoid(conv_gate.astype(jnp.float32))
    value_float = conv_value.astype(jnp.float32)
    gated_rows = lax.optimization_barrier((value_float * sig_gate).astype(jnp.bfloat16)).astype(jnp.float32)
    tap_reach = TAPS - 1
    padded_rows = jnp.pad(gated_rows, ((tap_reach, 0), (0, 0)))
    padded_grad = jnp.pad(height_grad, ((0, tap_reach), (0, 0)))
    tap_values = conv_taps.astype(jnp.float32)
    tap_list = []
    gated_grad = jnp.zeros_like(height_grad)
    for tap_index in range(TAPS):
        tap_list.append(lax.optimization_barrier(jnp.sum(height_grad * padded_rows[tap_index:tap_index + SEQ], axis=0)))
        begin = tap_reach - tap_index
        gated_grad = gated_grad + tap_values[tap_index] * padded_grad[begin:begin + SEQ]
    grad_taps = jnp.stack(tap_list)
    grad_value = (gated_grad * sig_gate).astype(jnp.bfloat16)
    grad_gate = (gated_grad * value_float * sig_gate * (1.0 - sig_gate)).astype(jnp.bfloat16)
    return (grad_value, grad_gate, grad_taps, grad_gain, grad_shift, grad_proj)
```

```python
import functools

import jax
import jax.numpy as jnp
from jax import lax
from jax.experimental import pallas as pl
from jax.experimental.pallas import tpu as pltpu
from jax.sharding import Mesh
from jax.sharding import PartitionSpec as P

SP = ("sp_0", "sp_1", "sp_2")
ALL = SP + ("tp",)
EPS = 1e-05
F32 = jnp.float32
BF16 = jnp.bfloat16
LANES = 128


def vmem(count):
    return [pl.BlockSpec(memory_space=pltpu.VMEM)] * count


def call(kernel, outs, *args, flops, name, scratch=(), specs=None):
    moved = sum(a.size * a.dtype.itemsize for a in args) + sum(
        o.size * o.dtype.itemsize for o in outs
    )
    return pl.pallas_call(
        kernel,
        out_shape=outs,
        in_specs=specs or vmem(len(args)),
        out_specs=vmem(len(outs)),
        scratch_shapes=list(scratch),
        cost_estimate=pl.CostEstimate(flops=flops, bytes_accessed=moved, transcendentals=0),
        compiler_params=pltpu.CompilerParams(vmem_limit_bytes=48 * 1024 * 1024),
        name=name,
    )(*args)


def shape(dims, dtype):
    return jax.ShapeDtypeStruct(dims, dtype)


def stats_kernel(conv_ref, out_ref):
    rows, chans = conv_ref.shape
    step = 64
    left = lax.broadcasted_iota(jnp.int32, (step, LANES), 1) < LANES // 2

    def body(i, carry):
        at = pl.ds(pl.multiple_of(i * step, step), step)
        x = conv_ref[at, :].astype(F32)
        total = jnp.sum(x, axis=1, keepdims=True)
        off = x - total * (1.0 / chans)
        spread = jnp.sum(off * off, axis=1, keepdims=True)
        out_ref[at, :] = jnp.where(left, total, spread)
        return carry

    lax.fori_loop(0, rows // step, body, 0)


def front_kernel(sizes, where_ref, grad_ref, weight_ref, act_grad_ref, turned_ref):
    nz, n1 = sizes
    pos1, pos2, stride1, stride2 = (where_ref[i] for i in range(4))
    rows, width = grad_ref.shape
    piece = width // (nz * n1 * n1)
    act_grad_ref[...] = jnp.dot(grad_ref[...], weight_ref[...], preferred_element_type=F32)
    span = LANES

    def body(b, carry):
        columns = pl.ds(pl.multiple_of(b * span, span), span)
        turned = grad_ref[:, columns].T
        for p in range(span // piece):
            at = b * (span // piece) + p
            c1 = lax.rem(at // stride1, n1)
            c2 = lax.rem(at // stride2, n1)
            z = at // (n1 * n1)
            k1 = lax.rem(c1 - pos1 + n1, n1)
            k2 = lax.rem(c2 - pos2 + n1, n1)
            to = ((k1 * n1 + k2) * nz + z) * piece
            turned_ref[pl.ds(pl.multiple_of(to, piece), piece), :] = turned[
                p * piece : (p + 1) * piece, :
            ]
        return carry

    lax.fori_loop(0, width // span, body, 0)


def norm_of(x, own, peer, chans):
    half = LANES // 2
    sum_a, dev_a = own[:, 0:1], own[:, half : half + 1]
    sum_b, dev_b = peer[:, 0:1], peer[:, half : half + 1]
    center = (sum_a + sum_b) * (0.5 / chans)
    apart = (sum_a - sum_b) * (1.0 / chans)
    variance = (dev_a + dev_b + apart * apart * (0.5 * chans)) * (0.5 / chans)
    inv_std = lax.rsqrt(variance + EPS)
    return (x - center) * inv_std, inv_std


def middle_kernel(
    conv_ref, own_ref, peer_ref, gain_ref, shift_ref, act_grad_ref,
    active_ref, scaled_ref, normed_ref, sums_ref, params_ref,
):
    rows, chans = conv_ref.shape
    step = 32
    gain, shift = gain_ref[...], shift_ref[...]
    left = lax.broadcasted_iota(jnp.int32, (step, LANES), 1) < LANES // 2

    def fold(x):
        return jnp.sum(x.reshape(step // 8, 8, chans), axis=0)

    def body(i, carry):
        gain_sum, shift_sum = carry
        at = pl.ds(pl.multiple_of(i * step, step), step)
        normed, _ = norm_of(conv_ref[at, :].astype(F32), own_ref[at, :], peer_ref[at, :], chans)
        shifted = normed * gain + shift
        sig = jax.nn.sigmoid(shifted)
        active_ref[at, :] = (shifted * sig).astype(BF16)
        norm_grad = act_grad_ref[at, :] * (sig * (1.0 + shifted * (1.0 - sig)))
        scaled = norm_grad * gain
        scaled_ref[at, :] = scaled
        normed_ref[at, :] = normed
        total = jnp.sum(scaled, axis=1, keepdims=True)
        dot = jnp.sum(scaled * normed, axis=1, keepdims=True)
        sums_ref[at, :] = jnp.where(left, total, dot)
        return gain_sum + fold(norm_grad * normed), shift_sum + fold(norm_grad)

    zero = jnp.zeros((8, chans), F32)
    gain_sum, shift_sum = lax.fori_loop(0, rows // step, body, (zero, zero))
    params_ref[0:1, :] = jnp.sum(gain_sum, axis=0, keepdims=True)
    params_ref[1:2, :] = jnp.sum(shift_sum, axis=0, keepdims=True)


def project_kernel(turned_ref, active_ref, *out_refs):
    rows = out_refs[0].shape[0]
    for k, out_ref in enumerate(out_refs):
        out_ref[...] = jnp.dot(
            turned_ref[k * rows : (k + 1) * rows, :], active_ref[...], preferred_element_type=F32
        ).astype(BF16)


def height_kernel(
    scaled_ref, normed_ref, own_ref, peer_ref, sums_ref, sums_peer_ref, height_ref, head_ref
):
    rows, chans = scaled_ref.shape
    step = 32
    half = LANES // 2

    def body(i, carry):
        at = pl.ds(pl.multiple_of(i * step, step), step)
        _, inv_std = norm_of(0.0, own_ref[at, :], peer_ref[at, :], chans)
        sums = (sums_ref[at, :] + sums_peer_ref[at, :]) * (0.5 / chans)
        height_ref[at, :] = inv_std * (
            scaled_ref[at, :] - sums[:, 0:1] - normed_ref[at, :] * sums[:, half : half + 1]
        )
        return carry

    lax.fori_loop(0, rows // step, body, 0)
    head_ref[...] = height_ref[0 : head_ref.shape[0], :]


def conv_kernel(
    value_ref, gate_ref, height_ref, halo_ref, taps_ref,
    grad_value_ref, grad_gate_ref, grad_taps_ref, moved, gated, sig_held, spread,
):
    rows = value_ref.shape[0]
    taps = taps_ref.shape[0]
    reach = taps - 1
    tail = halo_ref.shape[0]
    moved[0, 0:rows, :] = height_ref[...]
    moved[0, rows : rows + tail, :] = halo_ref[...]
    for s in range(1, 8):
        moved[s, 0 : rows + tail - 8, :] = moved[0, s : s + rows + tail - 8, :]
    sig = jax.nn.sigmoid(gate_ref[...].astype(F32))
    sig_held[...] = sig
    gated[...] = (value_ref[...].astype(F32) * sig).astype(BF16).astype(F32)
    for j in range(taps):
        spread[j] = jnp.broadcast_to(taps_ref[j : j + 1, :], (8, LANES))
    group = 2
    step = 8 * group

    def body(i, sums):
        at = pl.multiple_of(i * step, step)
        held = [gated[pl.ds(at + 8 * b, 8), :] for b in range(group)]
        total = [jnp.zeros((8, LANES), F32) for b in range(group)]
        out = []
        for j in range(taps):
            over = reach - j
            weight = spread[j]
            add = sums[j]
            for b in range(group):
                there = moved[over % 8, pl.ds(at + 8 * (b + over // 8), 8), :]
                total[b] = total[b] + weight * there
                add = add + held[b] * there
            out.append(add)
        for b in range(group):
            rows_at = pl.ds(at + 8 * b, 8)
            sig = sig_held[rows_at, :]
            spread_grad = total[b] * sig
            sig_held[rows_at, :] = spread_grad
            gated[rows_at, :] = spread_grad * (1.0 - sig)
        return tuple(out)

    zero = jnp.zeros((8, LANES), F32)
    sums = lax.fori_loop(0, rows // step, body, (zero,) * taps)
    for j in range(taps):
        grad_taps_ref[j : j + 1, :] = jnp.sum(sums[j], axis=0, keepdims=True)
    grad_taps_ref[taps:, :] = jnp.zeros((grad_taps_ref.shape[0] - taps, LANES), F32)
    grad_value_ref[...] = sig_held[...].astype(BF16)
    grad_gate_ref[...] = (gated[...] * value_ref[...].astype(F32)).astype(BF16)


def conv(value, gate, height, halo, taps, pad_taps):
    rows, chans = value.shape
    count = taps.shape[0]
    tail = halo.shape[0]

    def strip(n):
        return pl.BlockSpec((n, LANES), lambda i: (0, i))

    return pl.pallas_call(
        conv_kernel,
        grid=(chans // LANES,),
        out_shape=(
            shape((rows, chans), BF16),
            shape((rows, chans), BF16),
            shape((pad_taps, chans), F32),
        ),
        in_specs=[strip(rows), strip(rows), strip(rows), strip(tail), strip(count)],
        out_specs=[strip(rows), strip(rows), strip(pad_taps)],
        scratch_shapes=[
            pltpu.VMEM((8, rows + tail, LANES), F32),
            pltpu.VMEM((rows, LANES), F32),
            pltpu.VMEM((rows, LANES), F32),
            pltpu.VMEM((count, 8, LANES), F32),
        ],
        cost_estimate=pl.CostEstimate(
            flops=4 * count * rows * chans * 20, bytes_accessed=rows * chans * 12, transcendentals=0
        ),
        compiler_params=pltpu.CompilerParams(vmem_limit_bytes=48 * 1024 * 1024),
        name="conv",
    )(value, gate, height, halo, taps)


def gather_kernel(parts, extra, *refs):
    ins, outs = refs[: parts + extra], refs[parts + extra :]
    total = functools.reduce(lambda a, r: a + r[...].astype(F32), ins[1:parts], ins[0][...].astype(F32))
    rows = outs[0].shape[0] if not extra else total.shape[0] // len(outs)
    more = None
    if extra:
        more = functools.reduce(lambda a, r: a + r[...], ins[parts + 1 :], ins[parts][...]).astype(BF16)
    for k, out in enumerate(outs):
        out[0:rows, :] = total[k * rows : (k + 1) * rows, :].astype(BF16)
        if extra:
            out[rows:, :] = more


def local(conv_value, conv_gate, conv_out, conv_taps, norm_gain, norm_shift, proj_weight, out_grad):
    rows, chans = conv_value.shape
    width = out_grad.shape[1]
    taps = conv_taps.shape[0]
    nz, n1, n2, cores = (lax.axis_size(a) for a in ALL)
    tail = 32
    pad_taps = 48

    z, y, x, core = (lax.axis_index(a) for a in ALL)
    first = core == 0
    where = jnp.stack(
        [jnp.where(first, x, y), jnp.where(first, y, x), jnp.where(first, 1, n2), jnp.where(first, n2, 1)]
    ).astype(jnp.int32)

    def index(z, y, x, c):
        return ((z * n1 + y) * n2 + x) * cores + c

    everyone = [
        (z, y, x, c) for z in range(nz) for y in range(n1) for x in range(n2) for c in range(cores)
    ]

    def hop(array, k, stage):
        def to(z, y, x, c):
            along_x = (c == 0) == (stage == 1)
            return index(z, y, (x + k) % n2, c) if along_x else index(z, (y + k) % n1, x, c)

        return lax.ppermute(array, ALL, [(index(*d), to(*d)) for d in everyone])

    def other_core(array):
        return lax.ppermute(array, "tp", [(0, 1), (1, 0)])

    def previous(array):
        devices = range(nz * n1 * n2)
        return lax.ppermute(array, SP, [(i, i - 1) for i in devices if i])

    stats, = call(
        stats_kernel, (shape((rows, LANES), F32),), conv_out, flops=rows * chans * 100, name="stats"
    )
    stats_peer = other_core(stats)
    act_grad, turned = call(
        functools.partial(front_kernel, (nz, n1)),
        (shape((rows, chans), F32), shape((width, rows), BF16)),
        where, out_grad, proj_weight,
        flops=2 * rows * width * chans,
        name="front",
        specs=[pl.BlockSpec(memory_space=pltpu.SMEM)] + vmem(2),
    )
    active, scaled, normed, sums, params = call(
        middle_kernel,
        (
            shape((rows, chans), BF16), shape((rows, chans), F32), shape((rows, chans), F32),
            shape((rows, LANES), F32), shape((2, chans), F32),
        ),
        conv_out, stats, stats_peer, norm_gain[None], norm_shift[None], act_grad,
        flops=rows * chans * 1000,
        name="middle",
    )
    sums_peer = other_core(sums)
    blocks = call(
        project_kernel,
        (shape((width // n1, chans), BF16),) * n1,
        turned, active,
        flops=2 * rows * width * chans,
        name="project",
    )
    arrived = [blocks[0]] + [hop(blocks[k], k, 1) for k in range(1, n1)]
    height, head = call(
        height_kernel,
        (shape((rows, chans), F32), shape((tail, chans), F32)),
        scaled, normed, stats, stats_peer, sums, sums_peer,
        flops=rows * chans * 100,
        name="height",
    )
    halo = previous(head)
    grad_value, grad_gate, tap_rows = conv(
        conv_value, conv_gate, height, halo, conv_taps.astype(F32), 32
    )
    small = jnp.concatenate([tap_rows[:taps], params, jnp.zeros((pad_taps - taps - 2, chans), F32)])
    small_arrived = [small] + [hop(small, k, 1) for k in range(1, n1)]
    part = width // (n1 * n1)
    second = call(
        functools.partial(gather_kernel, n1, n1),
        (shape((part + pad_taps, chans), BF16),) * n1,
        *arrived, *small_arrived,
        flops=width * chans * 100,
        name="gather",
    )
    landed = [second[0]] + [hop(second[k], k, 2) for k in range(1, n1)]
    total = functools.reduce(lambda a, b: a + b, [a.astype(F32) for a in landed]).astype(BF16)
    own = part // nz
    small_total = total[part:]
    last = jnp.concatenate(
        [total[:part].reshape(nz, own, chans), jnp.broadcast_to(small_total[None], (nz, pad_taps, chans))],
        axis=1,
    )
    final = jnp.sum(lax.all_to_all(last, "sp_0", 0, 0).astype(F32), axis=0)
    grad_proj = final[:own]
    small_final = final[own:]
    return (
        grad_value, grad_gate, small_final[:taps], small_final[taps], small_final[taps + 1], grad_proj,
    )


def solution(mesh):
    split = Mesh(mesh.devices.reshape(8, 4, 4, mesh.shape["tp"]), ALL)
    placed = (
        P(SP, "tp"),
        P(SP, "tp"),
        P(SP, "tp"),
        P(None, "tp"),
        P("tp"),
        P("tp"),
        P(None, "tp"),
        P(SP, None),
    )
    return jax.shard_map(
        local,
        mesh=split,
        in_specs=placed,
        out_specs=(P(SP, "tp"), P(SP, "tp"), P(None, "tp"), P("tp"), P("tp"), P(SP, "tp")),
        check_vma=False,
    )
```

```python
import functools

import jax
import jax.numpy as jnp
from jax import lax
from jax.experimental import pallas as pl
from jax.experimental.pallas import tpu as pltpu
from jax.sharding import Mesh
from jax.sharding import PartitionSpec as P


SP = ("sp_0", "sp_1", "sp_2")
ALL = SP + ("tp",)
EPS = 1e-05
F32 = jnp.float32
BF16 = jnp.bfloat16
LANES = 128
MIB = 1024 * 1024


def vmem(count):
    return [pl.BlockSpec(memory_space=pltpu.VMEM)] * count


def call(kernel, outs, *args, flops, scratch=(), specs=None, limit=8):
    moved = sum(a.size * a.dtype.itemsize for a in args) + sum(
        o.size * o.dtype.itemsize for o in outs
    )
    return pl.pallas_call(
        kernel,
        out_shape=outs,
        in_specs=specs or vmem(len(args)),
        out_specs=vmem(len(outs)),
        scratch_shapes=list(scratch),
        cost_estimate=pl.CostEstimate(flops=flops, bytes_accessed=moved, transcendentals=0),
        compiler_params=pltpu.CompilerParams(vmem_limit_bytes=limit * MIB),
    )(*args)


def shape(dims, dtype):
    return jax.ShapeDtypeStruct(dims, dtype)


def left_half(rows):
    return lax.broadcasted_iota(jnp.int32, (rows, LANES), 1) < LANES // 2


def both(packed):
    left = left_half(packed.shape[0])
    turned = pltpu.roll(packed, LANES // 2, 1)
    return jnp.where(left, packed, turned), jnp.where(left, turned, packed)


def tiles(chans):
    return [slice(at, at + LANES) for at in range(0, chans, LANES)]


def front_kernel(
    place_ref, conv_hbm, grad_hbm, weight_hbm, stats_ref, act_grad_ref, conv_ref, grad_ref,
    weight_ref, conv_sem, grad_sem, weight_sem,
):
    loads = [
        pltpu.make_async_copy(conv_hbm, conv_ref, conv_sem),
        pltpu.make_async_copy(weight_hbm, weight_ref, weight_sem),
        pltpu.make_async_copy(grad_hbm, grad_ref, grad_sem),
    ]
    for load in loads:
        load.start()
    loads[0].wait()
    rows, chans = conv_ref.shape
    step = 128
    left = left_half(step)
    for begin in range(0, rows, step):
        at = slice(begin, begin + step)
        total = jnp.sum(
            sum(conv_ref[at, c].astype(F32) for c in tiles(chans)), axis=1, keepdims=True
        )
        mean = jnp.broadcast_to(total * (1.0 / chans), (step, LANES))
        spread = 0.0
        for c in tiles(chans):
            off = conv_ref[at, c].astype(F32) - mean
            spread = spread + off * off
        stats_ref[at, :] = jnp.where(left, total, jnp.sum(spread, axis=1, keepdims=True))
    for load in loads[1:]:
        load.wait()
    act_grad_ref[...] = jnp.dot(grad_ref[...], weight_ref[...], preferred_element_type=F32)


def turn_kernel(place_ref, grad_ref, turned_ref):
    _, width = grad_ref.shape
    piece = width // place_ref.shape[0]
    span = LANES
    each = span // piece

    def body(b, carry):
        columns = pl.ds(pl.multiple_of(b * span, span), span)
        turned = grad_ref[:, columns].T
        for p in range(each):
            to = place_ref[b * each + p]
            turned_ref[pl.ds(pl.multiple_of(to, piece), piece), :] = turned[
                p * piece : (p + 1) * piece, :
            ]
        return carry

    lax.fori_loop(0, width // span, body, 0, unroll=4)


def middle_kernel(
    conv_ref, own_ref, peer_ref, gain_ref, shift_ref, act_grad_ref,
    active_ref, lifted_ref, normed_ref, inv_ref, sums_ref, params_ref,
    center_ref, total_ref, dot_ref,
):
    rows, chans = conv_ref.shape
    wide = 128
    for begin in range(0, rows, wide):
        at = slice(begin, begin + wide)
        sum_a, dev_a = both(own_ref[at, :])
        sum_b, dev_b = both(peer_ref[at, :])
        apart = (sum_a - sum_b) * (1.0 / chans)
        variance = (dev_a + dev_b + apart * apart * (0.5 * chans)) * (0.5 / chans)
        center_ref[at, :] = (sum_a + sum_b) * (0.5 / chans)
        inv_ref[at, :] = lax.rsqrt(variance + EPS)
    step = 32

    def fold(x):
        return jnp.sum(x.reshape(step // 8, 8, LANES), axis=0)

    def body(i, carry):
        out = []
        at = pl.ds(pl.multiple_of(i * step, step), step)
        center, inv = center_ref[at, :], inv_ref[at, :]
        total, dot = 0.0, 0.0
        for k, c in enumerate(tiles(chans)):
            gain, shift = gain_ref[c].reshape(1, LANES), shift_ref[c].reshape(1, LANES)
            normed = (conv_ref[at, c].astype(F32) - center) * inv
            shifted = normed * gain + shift
            sig = jax.nn.sigmoid(shifted)
            active = shifted * sig
            active_ref[at, c] = active.astype(BF16)
            norm_grad = act_grad_ref[at, c] * (sig + active * (1.0 - sig))
            scaled = norm_grad * gain
            lifted_ref[at, c] = scaled * inv
            normed_ref[at, c] = normed
            total = total + scaled
            dot = dot + scaled * normed
            out.append(carry[2 * k] + fold(norm_grad * normed))
            out.append(carry[2 * k + 1] + fold(norm_grad))
        total_ref[at, :] = total
        dot_ref[at, :] = dot
        return tuple(out)

    zero = jnp.zeros((8, LANES), F32)
    folded = lax.fori_loop(0, rows // step, body, (zero,) * (2 * len(tiles(chans))))
    for k, c in enumerate(tiles(chans)):
        params_ref[0:1, c] = jnp.sum(folded[2 * k], axis=0, keepdims=True)
        params_ref[1:2, c] = jnp.sum(folded[2 * k + 1], axis=0, keepdims=True)
    left = left_half(wide)
    for begin in range(0, rows, wide):
        at = slice(begin, begin + wide)
        sums_ref[at, :] = jnp.where(
            left,
            jnp.sum(total_ref[at, :], axis=1, keepdims=True),
            jnp.sum(dot_ref[at, :], axis=1, keepdims=True),
        )


def project_kernel(turned_ref, active_ref, *out_refs):
    rows = out_refs[0].shape[0]
    for k, out_ref in enumerate(out_refs):
        out_ref[...] = jnp.dot(
            turned_ref[k * rows : (k + 1) * rows, :], active_ref[...], preferred_element_type=F32
        ).astype(BF16)


def head_kernel(
    lifted_ref, normed_ref, inv_ref, sums_ref, sums_peer_ref, mean_ref, slope_ref, head_ref
):
    rows, chans = lifted_ref.shape
    wide = 128
    for begin in range(0, rows, wide):
        at = slice(begin, begin + wide)
        total, dot = both(sums_ref[at, :] + sums_peer_ref[at, :])
        scale = inv_ref[at, :] * (0.5 / chans)
        mean_ref[at, :] = total * scale
        slope_ref[at, :] = dot * scale
    at = slice(0, head_ref.shape[0])
    for c in tiles(chans):
        head_ref[at, c] = lifted_ref[at, c] - mean_ref[at, :] - normed_ref[at, c] * slope_ref[at, :]


def fill_moved(moved, lanes, lifted_ref, normed_ref, mean_ref, slope_ref, halo_ref):
    rows = lifted_ref.shape[0]
    tail = halo_ref.shape[0]
    moved[0, 0:rows, :] = (
        lifted_ref[:, lanes] - mean_ref[...] - normed_ref[:, lanes] * slope_ref[...]
    )
    moved[0, rows : rows + tail, :] = halo_ref[:, lanes]
    for s in range(1, 8):
        moved[s, 0 : rows + tail - 8, :] = moved[0, s : s + rows + tail - 8, :]


def strips(body, chans):
    def step(i, carry):
        body(pl.ds(pl.multiple_of(i * LANES, LANES), LANES))
        return carry

    lax.fori_loop(0, chans // LANES, step, 0)


GROUP = 4


def taps_kernel(
    value_ref, gate_ref, lifted_ref, normed_ref, mean_ref, slope_ref, halo_ref, params_ref,
    out_ref, moved, gated, rows_ref,
):
    rows, chans = value_ref.shape
    taps = halo_ref.shape[0] - 1
    reach = taps - 1
    step = 8 * GROUP

    def one(lanes):
        fill_moved(moved, lanes, lifted_ref, normed_ref, mean_ref, slope_ref, halo_ref)
        sig = jax.nn.sigmoid(gate_ref[:, lanes].astype(F32))
        gated[...] = (value_ref[:, lanes].astype(F32) * sig).astype(BF16).astype(F32)

        def body(i, sums):
            at = pl.multiple_of(i * step, step)
            held = [gated[pl.ds(at + 8 * b, 8), :] for b in range(GROUP)]
            out = list(sums)
            for s in range(8):
                overs = range(s, taps, 8)
                there = [
                    moved[s, pl.ds(at + 8 * m, 8), :] for m in range(GROUP + len(overs) - 1)
                ]
                for q, over in enumerate(overs):
                    j = reach - over
                    products = [held[b] * there[b + q] for b in range(GROUP)]
                    out[j] = out[j] + ((products[0] + products[1]) + (products[2] + products[3]))
            return tuple(out)

        zero = jnp.zeros((8, LANES), F32)
        sums = lax.fori_loop(0, rows // step, body, (zero,) * taps)
        for j in range(taps):
            rows_ref[j : j + 1, :] = jnp.sum(sums[j], axis=0, keepdims=True)
        rows_ref[taps : taps + 2, :] = params_ref[:, lanes]
        rows_ref[taps + 2 :, :] = jnp.zeros((rows_ref.shape[0] - taps - 2, LANES), F32)
        out_ref[:, lanes] = rows_ref[...].astype(BF16)

    strips(one, chans)


def spread_kernel(
    value_ref, gate_ref, lifted_ref, normed_ref, mean_ref, slope_ref, halo_ref, taps_ref,
    grad_value_ref, grad_gate_ref, moved, spread,
):
    rows, chans = value_ref.shape
    taps = taps_ref.shape[0]
    reach = taps - 1
    step = 8 * GROUP

    def one(lanes):
        fill_moved(moved, lanes, lifted_ref, normed_ref, mean_ref, slope_ref, halo_ref)
        weights = taps_ref[:, lanes].astype(F32)
        for j in range(taps):
            spread[j] = jnp.broadcast_to(weights[j : j + 1, :], (8, LANES))

        def body(i, carry):
            at = pl.multiple_of(i * step, step)
            total = [None] * GROUP
            for s in range(8):
                overs = range(s, taps, 8)
                there = [
                    moved[s, pl.ds(at + 8 * m, 8), :] for m in range(GROUP + len(overs) - 1)
                ]
                for q, over in enumerate(overs):
                    weight = spread[reach - over]
                    for b in range(GROUP):
                        term = weight * there[b + q]
                        total[b] = term if total[b] is None else total[b] + term
            here = pl.ds(at, step)
            gated_grad = jnp.concatenate(total, axis=0)
            sig = jax.nn.sigmoid(gate_ref[here, lanes].astype(F32))
            grad_value = gated_grad * sig
            grad_value_ref[here, lanes] = grad_value.astype(BF16)
            grad_gate_ref[here, lanes] = (
                grad_value * value_ref[here, lanes].astype(F32) * (1.0 - sig)
            ).astype(BF16)
            return carry

        lax.fori_loop(0, rows // step, body, 0)

    strips(one, chans)


def added(refs, at=slice(None)):
    return functools.reduce(lambda a, b: a + b, [r[at, :].astype(F32) for r in refs])


def second_kernel(n, *refs):
    landed, small, outs = refs[:n], refs[n : 2 * n], refs[2 * n :]
    rows = landed[0].shape[0] // n
    more = added(small).astype(BF16)
    for k, out in enumerate(outs):
        out[0:rows, :] = added(landed, slice(k * rows, (k + 1) * rows)).astype(BF16)
        out[rows:, :] = more


def third_kernel(*refs):
    landed, (keep_ref, send_ref) = refs[:-2], refs[-2:]
    rows = keep_ref.shape[0]
    keep_ref[...] = added(landed, slice(0, rows))
    send_ref[...] = added(landed, slice(rows, None)).astype(BF16)


def fourth_kernel(keep_ref, sent_ref, came_ref, *outs):
    rows = keep_ref.shape[0]
    own = rows // len(outs)
    small = added((sent_ref, came_ref), slice(rows, None)).astype(BF16)
    for k, out in enumerate(outs):
        at = slice(k * own, (k + 1) * own)
        out[0:own, :] = added((keep_ref, came_ref), at).astype(out.dtype)
        out[own:, :] = small.astype(out.dtype)


def last_kernel(taps, *refs):
    landed, (project_ref, taps_ref, params_ref) = refs[:-3], refs[-3:]
    own = project_ref.shape[0]
    total = added(landed)
    project_ref[...] = total[:own, :]
    taps_ref[...] = total[own : own + taps, :]
    params_ref[...] = total[own + taps : own + taps + 2, :]


def local(conv_value, conv_gate, conv_out, conv_taps, norm_gain, norm_shift, proj_weight, out_grad):
    rows, chans = conv_value.shape
    width = out_grad.shape[1]
    taps = conv_taps.shape[0]
    nz, n, _, cores = (lax.axis_size(a) for a in ALL)
    tail = taps + 1
    extra = -(-(taps + 2) // 8) * 8
    own = width // (nz * n * n)

    z, y, x, core = (lax.axis_index(a) for a in ALL)
    group = lax.iota(jnp.int32, nz * n * n)
    away_y, away_x = (group // n + n - y) % n, (group + n - x) % n
    to_z = group // (n * n)
    away_z = (to_z + nz - z) % nz
    odd = (to_z + z) % 2
    slot_z = odd * (nz // 2) + jnp.where(odd == 1, (to_z + nz - (z ^ 1)) % nz, away_z) // 2
    ahead = jnp.where(core == 0, away_x, away_y) * n + jnp.where(core == 0, away_y, away_x)
    place = (ahead * nz + slot_z) * own

    places = [
        (z, y, x, c) for z in range(nz) for y in range(n) for x in range(n) for c in range(cores)
    ]

    def index(z, y, x, c):
        return ((z * n + y) * n + x) * cores + c

    def hop(array, k, stage):
        def to(z, y, x, c):
            if (c == 0) == (stage == 1):
                return index(z, y, (x + k) % n, c)
            return index(z, (y + k) % n, x, c)

        return lax.ppermute(array, ALL, [(index(*at), to(*at)) for at in places])

    def hop_z(array, k):
        return lax.ppermute(array, "sp_0", [(i, (i + k) % nz) for i in range(nz)])

    def swap_z(array):
        return lax.ppermute(array, "sp_0", [(i, i ^ 1) for i in range(nz)])

    def other_core(array):
        return lax.ppermute(array, "tp", [(0, 1), (1, 0)])

    def previous(array):
        return lax.ppermute(array, SP, [(i, i - 1) for i in range(1, nz * n * n)])

    stats, act_grad, height, grads = call(
        front_kernel,
        (
            shape((rows, LANES), F32), shape((rows, chans), F32),
            shape(conv_out.shape, BF16), shape(out_grad.shape, BF16),
        ),
        place, *(pltpu.with_memory_space_constraint(a, pltpu.HBM) for a in (conv_out, out_grad, proj_weight)),
        flops=2 * rows * width * chans,
        scratch=[pltpu.VMEM(proj_weight.shape, BF16)] + [pltpu.SemaphoreType.DMA] * 3,
        specs=[pl.BlockSpec(memory_space=pltpu.SMEM)] + [pl.BlockSpec(memory_space=pltpu.HBM)] * 3,
        limit=12,
    )
    stats_peer = other_core(stats)
    (turned,) = call(
        turn_kernel,
        (shape((width, rows), BF16),),
        place, grads,
        flops=rows * width * chans,
        specs=[pl.BlockSpec(memory_space=pltpu.SMEM)] + vmem(1),
        limit=4,
    )
    active, lifted, normed, inv, sums, params = call(
        middle_kernel,
        (
            shape((rows, chans), BF16), shape((rows, chans), F32), shape((rows, chans), F32),
            shape((rows, LANES), F32), shape((rows, LANES), F32), shape((2, chans), F32),
        ),
        height, stats, stats_peer, norm_gain, norm_shift, act_grad,
        flops=rows * chans * 1000,
        scratch=[pltpu.VMEM((rows, LANES), F32)] * 3,
    )
    sums_peer = other_core(sums)
    blocks = call(
        project_kernel,
        (shape((width // n, chans), BF16),) * n,
        turned, active,
        flops=2 * rows * width * chans,
    )
    mean, slope, head = call(
        head_kernel,
        (shape((rows, LANES), F32), shape((rows, LANES), F32), shape((tail, chans), F32)),
        lifted, normed, inv, sums, sums_peer,
        flops=rows * chans * 10,
    )
    halo = previous(head)
    landed = [blocks[0]] + [hop(blocks[k], k, 1) for k in range(1, n)]
    heights = (lifted, normed, mean, slope, halo)
    (small,) = call(
        taps_kernel,
        (shape((extra, chans), BF16),),
        conv_value, conv_gate, *heights, params,
        flops=taps * rows * chans * 40,
        scratch=[pltpu.VMEM((8, rows + tail, LANES), F32), pltpu.VMEM((rows, LANES), F32),
            pltpu.VMEM((extra, LANES), F32),
        ],
    )
    grad_value, grad_gate = call(
        spread_kernel,
        (shape((rows, chans), BF16),) * 2,
        conv_value, conv_gate, *heights, conv_taps,
        flops=taps * rows * chans * 40,
        scratch=[pltpu.VMEM((8, rows + tail, LANES), F32), pltpu.VMEM((taps, 8, LANES), F32)],
    )
    smalls = [small] + [hop(small, k, 1) for k in range(1, n)]
    part = width // (n * n)
    second = call(
        functools.partial(second_kernel, n),
        (shape((part + extra, chans), BF16),) * n,
        *landed, *smalls,
        flops=width * chans * 100,
    )
    then = [second[0]] + [hop(second[k], k, 2) for k in range(1, n)]
    keep, send = call(
        third_kernel,
        (shape((part // 2, chans), F32), shape((part // 2 + extra, chans), BF16)),
        *then,
        flops=width * chans * 10,
    )
    came = swap_z(send)
    fourth = call(
        fourth_kernel,
        (shape((own + extra, chans), F32),) + (shape((own + extra, chans), BF16),) * (nz // 2 - 1),
        keep, send, came,
        flops=width * chans * 10,
    )
    fars = [fourth[0]] + [hop_z(fourth[k], 2 * k) for k in range(1, nz // 2)]
    grad_proj, grad_taps, grad_params = call(
        functools.partial(last_kernel, taps),
        (shape((own, chans), F32), shape((taps, chans), F32), shape((2, chans), F32)),
        *fars,
        flops=width * chans * 10,
    )
    return grad_value, grad_gate, grad_taps, grad_params[0], grad_params[1], grad_proj


def solution(mesh):
    split = Mesh(mesh.devices.reshape(8, 4, 4, mesh.shape["tp"]), ALL)
    placed = (
        P(SP, "tp"),
        P(SP, "tp"),
        P(SP, "tp"),
        P(None, "tp"),
        P("tp"),
        P("tp"),
        P(None, "tp"),
        P(SP, None),
    )
    return jax.shard_map(
        local,
        mesh=split,
        in_specs=placed,
        out_specs=(P(SP, "tp"), P(SP, "tp"), P(None, "tp"), P("tp"), P("tp"), P(SP, "tp")),
        check_vma=False,
    )
```

```python
import functools

import jax
import jax.numpy as jnp
from jax import lax
from jax.experimental import pallas as pl
from jax.experimental.pallas import tpu as pltpu
from jax.sharding import Mesh
from jax.sharding import PartitionSpec as P


SP = ("sp_0", "sp_1", "sp_2")
ALL = SP + ("tp",)
EPS = 1e-05
F32 = jnp.float32
BF16 = jnp.bfloat16
LANES = 128
MIB = 1024 * 1024


def vmem(count):
    return [pl.BlockSpec(memory_space=pltpu.VMEM)] * count


def call(kernel, outs, *args, flops, scratch=(), specs=None, limit=8):
    moved = sum(a.size * a.dtype.itemsize for a in args) + sum(
        o.size * o.dtype.itemsize for o in outs
    )
    return pl.pallas_call(
        kernel,
        out_shape=outs,
        in_specs=specs or vmem(len(args)),
        out_specs=vmem(len(outs)),
        scratch_shapes=list(scratch),
        cost_estimate=pl.CostEstimate(flops=flops, bytes_accessed=moved, transcendentals=0),
        compiler_params=pltpu.CompilerParams(vmem_limit_bytes=limit * MIB),
    )(*args)


def shape(dims, dtype):
    return jax.ShapeDtypeStruct(dims, dtype)


def left_half(rows):
    return lax.broadcasted_iota(jnp.int32, (rows, LANES), 1) < LANES // 2


def both(packed):
    left = left_half(packed.shape[0])
    turned = pltpu.roll(packed, LANES // 2, 1)
    return jnp.where(left, packed, turned), jnp.where(left, turned, packed)


def tiles(chans):
    return [slice(at, at + LANES) for at in range(0, chans, LANES)]


def front_kernel(
    place_ref, conv_hbm, grad_hbm, weight_hbm, stats_ref, act_grad_ref, conv_ref, grad_ref,
    weight_ref, conv_sem, grad_sem, weight_sems,
):
    parts = weight_sems.shape[0]
    wide = weight_ref.shape[1] // parts
    columns = [slice(k * wide, (k + 1) * wide) for k in range(parts)]
    loads = [
        pltpu.make_async_copy(conv_hbm, conv_ref, conv_sem),
        pltpu.make_async_copy(grad_hbm, grad_ref, grad_sem),
    ]
    for k, c in enumerate(columns):
        loads.append(
            pltpu.make_async_copy(weight_hbm.at[:, c], weight_ref.at[:, c], weight_sems.at[k])
        )
    for load in loads:
        load.start()
    loads[0].wait()
    rows, chans = conv_ref.shape
    step = 128
    left = left_half(step)
    for begin in range(0, rows, step):
        at = slice(begin, begin + step)
        total = jnp.sum(
            sum(conv_ref[at, c].astype(F32) for c in tiles(chans)), axis=1, keepdims=True
        )
        mean = jnp.broadcast_to(total * (1.0 / chans), (step, LANES))
        spread = 0.0
        for c in tiles(chans):
            off = conv_ref[at, c].astype(F32) - mean
            spread = spread + off * off
        stats_ref[at, :] = jnp.where(left, total, jnp.sum(spread, axis=1, keepdims=True))
    loads[1].wait()
    for load, c in zip(loads[2:], columns):
        load.wait()
        act_grad_ref[:, c] = jnp.dot(grad_ref[...], weight_ref[:, c], preferred_element_type=F32)


def turn_kernel(place_ref, grad_ref, turned_ref):
    _, width = grad_ref.shape
    piece = width // place_ref.shape[0]
    span = LANES
    each = span // piece

    def body(b, carry):
        columns = pl.ds(pl.multiple_of(b * span, span), span)
        turned = grad_ref[:, columns].T
        for p in range(each):
            to = place_ref[b * each + p]
            turned_ref[pl.ds(pl.multiple_of(to, piece), piece), :] = turned[
                p * piece : (p + 1) * piece, :
            ]
        return carry

    lax.fori_loop(0, width // span, body, 0, unroll=4)


def middle_kernel(
    conv_ref, own_ref, peer_ref, gain_ref, shift_ref, act_grad_ref,
    active_ref, lifted_ref, normed_ref, inv_ref, sums_ref, params_ref,
    center_ref, total_ref, dot_ref,
):
    rows, chans = conv_ref.shape
    wide = 128
    for begin in range(0, rows, wide):
        at = slice(begin, begin + wide)
        sum_a, dev_a = both(own_ref[at, :])
        sum_b, dev_b = both(peer_ref[at, :])
        apart = (sum_a - sum_b) * (1.0 / chans)
        variance = (dev_a + dev_b + apart * apart * (0.5 * chans)) * (0.5 / chans)
        center_ref[at, :] = (sum_a + sum_b) * (0.5 / chans)
        inv_ref[at, :] = lax.rsqrt(variance + EPS)
    step = 32

    def fold(x):
        return jnp.sum(x.reshape(step // 8, 8, LANES), axis=0)

    def body(i, carry):
        out = []
        at = pl.ds(pl.multiple_of(i * step, step), step)
        center, inv = center_ref[at, :], inv_ref[at, :]
        total, dot = 0.0, 0.0
        for k, c in enumerate(tiles(chans)):
            gain, shift = gain_ref[c].reshape(1, LANES), shift_ref[c].reshape(1, LANES)
            normed = (conv_ref[at, c].astype(F32) - center) * inv
            shifted = normed * gain + shift
            sig = jax.nn.sigmoid(shifted)
            active = shifted * sig
            active_ref[at, c] = active.astype(BF16)
            norm_grad = act_grad_ref[at, c] * (sig + active * (1.0 - sig))
            scaled = norm_grad * gain
            lifted_ref[at, c] = scaled * inv
            normed_ref[at, c] = normed
            total = total + scaled
            dot = dot + scaled * normed
            out.append(carry[2 * k] + fold(norm_grad * normed))
            out.append(carry[2 * k + 1] + fold(norm_grad))
        total_ref[at, :] = total
        dot_ref[at, :] = dot
        return tuple(out)

    zero = jnp.zeros((8, LANES), F32)
    folded = lax.fori_loop(0, rows // step, body, (zero,) * (2 * len(tiles(chans))))
    for k, c in enumerate(tiles(chans)):
        params_ref[0:1, c] = jnp.sum(folded[2 * k], axis=0, keepdims=True)
        params_ref[1:2, c] = jnp.sum(folded[2 * k + 1], axis=0, keepdims=True)
    left = left_half(wide)
    for begin in range(0, rows, wide):
        at = slice(begin, begin + wide)
        sums_ref[at, :] = jnp.where(
            left,
            jnp.sum(total_ref[at, :], axis=1, keepdims=True),
            jnp.sum(dot_ref[at, :], axis=1, keepdims=True),
        )


def project_kernel(turned_ref, active_ref, *out_refs):
    rows = out_refs[0].shape[0]
    for k, out_ref in enumerate(out_refs):
        out_ref[...] = jnp.dot(
            turned_ref[k * rows : (k + 1) * rows, :], active_ref[...], preferred_element_type=F32
        ).astype(BF16)


def head_kernel(
    lifted_ref, normed_ref, inv_ref, sums_ref, sums_peer_ref, mean_ref, slope_ref, head_ref
):
    rows, chans = lifted_ref.shape
    wide = 128
    for begin in range(0, rows, wide):
        at = slice(begin, begin + wide)
        total, dot = both(sums_ref[at, :] + sums_peer_ref[at, :])
        scale = inv_ref[at, :] * (0.5 / chans)
        mean_ref[at, :] = total * scale
        slope_ref[at, :] = dot * scale
    at = slice(0, head_ref.shape[0])
    for c in tiles(chans):
        head_ref[at, c] = lifted_ref[at, c] - mean_ref[at, :] - normed_ref[at, c] * slope_ref[at, :]


def fill_heights(heights, lanes, lifted_ref, normed_ref, mean_ref, slope_ref, halo_ref):
    rows = lifted_ref.shape[0]
    tail = halo_ref.shape[0]
    heights[0:rows, :] = (
        lifted_ref[:, lanes] - mean_ref[...] - normed_ref[:, lanes] * slope_ref[...]
    )
    heights[rows : rows + tail, :] = halo_ref[:, lanes]


def strips(body, begin, end):
    def step(i, carry):
        body(i * LANES)
        return carry

    lax.fori_loop(begin // LANES, end // LANES, step, 0)


def lanes_at(at):
    return pl.ds(pl.multiple_of(at, LANES), LANES)


GROUP = 4


def taps_kernel(
    value_ref, gate_ref, lifted_ref, normed_ref, mean_ref, slope_ref, halo_ref, params_ref,
    out_ref, heights, gated, rows_ref,
):
    rows, chans = value_ref.shape
    taps = halo_ref.shape[0] - 1
    reach = taps - 1
    step = 8 * GROUP

    def one(lanes):
        fill_heights(heights, lanes, lifted_ref, normed_ref, mean_ref, slope_ref, halo_ref)
        sig = jax.nn.sigmoid(gate_ref[:, lanes].astype(F32))
        gated[...] = (value_ref[:, lanes].astype(F32) * sig).astype(BF16).astype(F32)

        def body(i, sums):
            at = pl.multiple_of(i * step, step)
            held = [gated[pl.ds(at + 8 * b, 8), :] for b in range(GROUP)]
            out = list(sums)
            for s in range(8):
                overs = range(s, taps, 8)
                there = [
                    heights[pl.ds(at + (8 * m + s), 8), :] for m in range(GROUP + len(overs) - 1)
                ]
                for q, over in enumerate(overs):
                    j = reach - over
                    products = [held[b] * there[b + q] for b in range(GROUP)]
                    out[j] = out[j] + ((products[0] + products[1]) + (products[2] + products[3]))
            return tuple(out)

        zero = jnp.zeros((8, LANES), F32)
        sums = lax.fori_loop(0, rows // step, body, (zero,) * taps)
        for j in range(taps):
            rows_ref[j : j + 1, :] = jnp.sum(sums[j], axis=0, keepdims=True)
        rows_ref[taps : taps + 2, :] = params_ref[:, lanes]
        rows_ref[taps + 2 :, :] = jnp.zeros((rows_ref.shape[0] - taps - 2, LANES), F32)
        out_ref[:, lanes] = rows_ref[...].astype(BF16)

    strips(lambda at: one(lanes_at(at)), 0, chans)


def spread_kernel(
    begin, value_ref, gate_ref, lifted_ref, normed_ref, mean_ref, slope_ref, halo_ref, taps_ref, *refs
):
    grad_value_ref, grad_gate_ref, heights, spread = refs[-4:]
    rows = value_ref.shape[0]
    taps = taps_ref.shape[0]
    reach = taps - 1
    step = 8 * GROUP

    def one(at_lane):
        lanes, there_lanes = lanes_at(at_lane), lanes_at(at_lane - begin)
        fill_heights(heights, lanes, lifted_ref, normed_ref, mean_ref, slope_ref, halo_ref)
        weights = taps_ref[:, lanes].astype(F32)
        for j in range(taps):
            spread[j] = jnp.broadcast_to(weights[j : j + 1, :], (8, LANES))

        def body(i, carry):
            at = pl.multiple_of(i * step, step)
            total = [None] * GROUP
            for s in range(8):
                overs = range(s, taps, 8)
                there = [
                    heights[pl.ds(at + (8 * m + s), 8), :] for m in range(GROUP + len(overs) - 1)
                ]
                for q, over in enumerate(overs):
                    weight = spread[reach - over]
                    for b in range(GROUP):
                        term = weight * there[b + q]
                        total[b] = term if total[b] is None else total[b] + term
            here = pl.ds(at, step)
            gated_grad = jnp.concatenate(total, axis=0)
            sig = jax.nn.sigmoid(gate_ref[here, lanes].astype(F32))
            grad_value = gated_grad * sig
            grad_value_ref[here, there_lanes] = grad_value.astype(BF16)
            grad_gate_ref[here, there_lanes] = (
                grad_value * value_ref[here, lanes].astype(F32) * (1.0 - sig)
            ).astype(BF16)
            return carry

        lax.fori_loop(0, rows // step, body, 0)

    strips(one, begin, begin + grad_value_ref.shape[1])


def added(refs, at=slice(None)):
    return functools.reduce(lambda a, b: a + b, [r[at, :].astype(F32) for r in refs])


def second_kernel(n, *refs):
    landed, small, outs = refs[:n], refs[n : 2 * n], refs[2 * n :]
    rows = landed[0].shape[0] // n
    more = added(small).astype(BF16)
    for k, out in enumerate(outs):
        out[0:rows, :] = added(landed, slice(k * rows, (k + 1) * rows)).astype(BF16)
        out[rows:, :] = more


def third_kernel(*refs):
    landed, (keep_ref, send_ref) = refs[:-2], refs[-2:]
    rows = keep_ref.shape[0]
    keep_ref[...] = added(landed, slice(0, rows))
    send_ref[...] = added(landed, slice(rows, None)).astype(BF16)


def fourth_kernel(keep_ref, sent_ref, came_ref, *outs):
    rows = keep_ref.shape[0]
    own = rows // len(outs)
    small = added((sent_ref, came_ref), slice(rows, None)).astype(BF16)
    for k, out in enumerate(outs):
        at = slice(k * own, (k + 1) * own)
        out[0:own, :] = added((keep_ref, came_ref), at).astype(out.dtype)
        out[own:, :] = small.astype(out.dtype)


def last_kernel(taps, *refs):
    landed, (project_ref, taps_ref, gain_ref, shift_ref) = refs[:-4], refs[-4:]
    own = project_ref.shape[0]
    total = added(landed)
    project_ref[...] = total[:own, :]
    taps_ref[...] = total[own : own + taps, :]
    gain_ref[...] = total[own + taps, :]
    shift_ref[...] = total[own + taps + 1, :]


def local(conv_value, conv_gate, conv_out, conv_taps, norm_gain, norm_shift, proj_weight, out_grad):
    rows, chans = conv_value.shape
    width = out_grad.shape[1]
    taps = conv_taps.shape[0]
    nz, n, _, cores = (lax.axis_size(a) for a in ALL)
    tail = taps + 1
    extra = -(-(taps + 2) // 8) * 8
    own = width // (nz * n * n)

    z, y, x, core = (lax.axis_index(a) for a in ALL)
    group = lax.iota(jnp.int32, nz * n * n)
    away_y, away_x = (group // n + n - y) % n, (group + n - x) % n
    to_z = group // (n * n)
    away_z = (to_z + nz - z) % nz
    odd = (to_z + z) % 2
    slot_z = odd * (nz // 2) + jnp.where(odd == 1, (to_z + nz - (z ^ 1)) % nz, away_z) // 2
    ahead = jnp.where(core == 0, away_x, away_y) * n + jnp.where(core == 0, away_y, away_x)
    place = (ahead * nz + slot_z) * own

    places = [
        (z, y, x, c) for z in range(nz) for y in range(n) for x in range(n) for c in range(cores)
    ]

    def index(z, y, x, c):
        return ((z * n + y) * n + x) * cores + c

    def hop(array, k, stage):
        def to(z, y, x, c):
            if (c == 0) == (stage == 1):
                return index(z, y, (x + k) % n, c)
            return index(z, (y + k) % n, x, c)

        return lax.ppermute(array, ALL, [(index(*at), to(*at)) for at in places])

    def hop_z(array, k):
        return lax.ppermute(array, "sp_0", [(i, (i + k) % nz) for i in range(nz)])

    def swap_z(array):
        return lax.ppermute(array, "sp_0", [(i, i ^ 1) for i in range(nz)])

    def other_core(array):
        return lax.ppermute(array, "tp", [(0, 1), (1, 0)])

    def previous(array):
        return lax.ppermute(array, SP, [(i, i - 1) for i in range(1, nz * n * n)])

    stats, act_grad, height, grads = call(
        front_kernel,
        (
            shape((rows, LANES), F32), shape((rows, chans), F32),
            shape(conv_out.shape, BF16), shape(out_grad.shape, BF16),
        ),
        place, *(pltpu.with_memory_space_constraint(a, pltpu.HBM) for a in (conv_out, out_grad, proj_weight)),
        flops=2 * rows * width * chans,
        scratch=[
            pltpu.VMEM(proj_weight.shape, BF16),
            pltpu.SemaphoreType.DMA,
            pltpu.SemaphoreType.DMA,
            pltpu.SemaphoreType.DMA((3,)),
        ],
        specs=[pl.BlockSpec(memory_space=pltpu.SMEM)] + [pl.BlockSpec(memory_space=pltpu.HBM)] * 3,
        limit=12,
    )
    stats_peer = other_core(stats)
    (turned,) = call(
        turn_kernel,
        (shape((width, rows), BF16),),
        place, grads,
        flops=rows * width * chans,
        specs=[pl.BlockSpec(memory_space=pltpu.SMEM)] + vmem(1),
        limit=4,
    )
    active, lifted, normed, inv, sums, params = call(
        middle_kernel,
        (
            shape((rows, chans), BF16), shape((rows, chans), F32), shape((rows, chans), F32),
            shape((rows, LANES), F32), shape((rows, LANES), F32), shape((2, chans), F32),
        ),
        height, stats, stats_peer, norm_gain, norm_shift, act_grad,
        flops=rows * chans * 1000,
        scratch=[pltpu.VMEM((rows, LANES), F32)] * 3,
    )
    sums_peer = other_core(sums)
    blocks = call(
        project_kernel,
        (shape((width // n, chans), BF16),) * n,
        turned, active,
        flops=2 * rows * width * chans,
    )
    mean, slope, head = call(
        head_kernel,
        (shape((rows, LANES), F32), shape((rows, LANES), F32), shape((tail, chans), F32)),
        lifted, normed, inv, sums, sums_peer,
        flops=rows * chans * 10,
    )
    halo = previous(head)
    landed = [blocks[0]] + [hop(blocks[k], k, 1) for k in range(1, n)]
    heights = (lifted, normed, mean, slope, halo)
    (small,) = call(
        taps_kernel,
        (shape((extra, chans), BF16),),
        conv_value, conv_gate, *heights, params,
        flops=taps * rows * chans * 40,
        scratch=[pltpu.VMEM((rows + tail, LANES), F32), pltpu.VMEM((rows, LANES), F32),
            pltpu.VMEM((extra, LANES), F32),
        ],
    )

    def spread_part(part, before):
        half = chans // 2
        operands = (conv_value, conv_gate, *heights, conv_taps)
        block = pl.BlockSpec((rows, half), lambda i: (0, part))
        return pl.pallas_call(
            functools.partial(spread_kernel, part * half),
            grid=(1,),
            out_shape=(shape((rows, chans), BF16),) * 2,
            in_specs=vmem(len(operands)) + [pl.BlockSpec(memory_space=pl.ANY)] * len(before),
            out_specs=(block, block),
            input_output_aliases={len(operands) + k: k for k in range(len(before))},
            scratch_shapes=[
                pltpu.VMEM((rows + tail, LANES), F32), pltpu.VMEM((taps, 8, LANES), F32),
            ],
            cost_estimate=pl.CostEstimate(
                flops=taps * rows * chans * 20, bytes_accessed=rows * chans * 10, transcendentals=0
            ),
            compiler_params=pltpu.CompilerParams(vmem_limit_bytes=8 * MIB),
            name="spread",
        )(*operands, *before)

    halves = spread_part(0, ())
    grad_value, grad_gate = spread_part(1, halves)
    smalls = [small] + [hop(small, k, 1) for k in range(1, n)]
    part = width // (n * n)
    second = call(
        functools.partial(second_kernel, n),
        (shape((part + extra, chans), BF16),) * n,
        *landed, *smalls,
        flops=width * chans * 100,
    )
    then = [second[0]] + [hop(second[k], k, 2) for k in range(1, n)]
    keep, send = call(
        third_kernel,
        (shape((part // 2, chans), F32), shape((part // 2 + extra, chans), BF16)),
        *then,
        flops=width * chans * 10,
    )
    came = swap_z(send)
    fourth = call(
        fourth_kernel,
        (shape((own + extra, chans), F32),) + (shape((own + extra, chans), BF16),) * (nz // 2 - 1),
        keep, send, came,
        flops=width * chans * 10,
    )
    fars = [fourth[0]] + [hop_z(fourth[k], 2 * k) for k in range(1, nz // 2)]
    grad_proj, grad_taps, grad_gain, grad_shift = call(
        functools.partial(last_kernel, taps),
        (shape((own, chans), F32), shape((taps, chans), F32), shape((chans,), F32), shape((chans,), F32)),
        *fars,
        flops=width * chans * 10,
    )
    return grad_value, grad_gate, grad_taps, grad_gain, grad_shift, grad_proj


def solution(mesh):
    split = Mesh(mesh.devices.reshape(8, 4, 4, mesh.shape["tp"]), ALL)
    placed = (
        P(SP, "tp"),
        P(SP, "tp"),
        P(SP, "tp"),
        P(None, "tp"),
        P("tp"),
        P("tp"),
        P(None, "tp"),
        P(SP, None),
    )
    return jax.shard_map(
        local,
        mesh=split,
        in_specs=placed,
        out_specs=(P(SP, "tp"), P(SP, "tp"), P(None, "tp"), P("tp"), P("tp"), P(SP, "tp")),
        check_vma=False,
    )
```

```python
import functools

import jax
import jax.numpy as jnp
from jax import lax
from jax.experimental import pallas as pl
from jax.experimental.pallas import tpu as pltpu
from jax.sharding import Mesh
from jax.sharding import PartitionSpec as P


SP = ("sp_0", "sp_1", "sp_2")
ALL = SP + ("tp",)
EPS = 1e-05
F32 = jnp.float32
BF16 = jnp.bfloat16
LANES = 128
MIB = 1024 * 1024


def vmem(count):
    return [pl.BlockSpec(memory_space=pltpu.VMEM)] * count


def call(kernel, outs, *args, flops, scratch=(), specs=None, limit=8):
    moved = sum(a.size * a.dtype.itemsize for a in args) + sum(
        o.size * o.dtype.itemsize for o in outs
    )
    return pl.pallas_call(
        kernel,
        out_shape=outs,
        in_specs=specs or vmem(len(args)),
        out_specs=vmem(len(outs)),
        scratch_shapes=list(scratch),
        cost_estimate=pl.CostEstimate(flops=flops, bytes_accessed=moved, transcendentals=0),
        compiler_params=pltpu.CompilerParams(vmem_limit_bytes=limit * MIB),
    )(*args)


def shape(dims, dtype):
    return jax.ShapeDtypeStruct(dims, dtype)


def left_half(rows):
    return lax.broadcasted_iota(jnp.int32, (rows, LANES), 1) < LANES // 2


def both(packed):
    left = left_half(packed.shape[0])
    turned = pltpu.roll(packed, LANES // 2, 1)
    return jnp.where(left, packed, turned), jnp.where(left, turned, packed)


def tiles(chans):
    return [slice(at, at + LANES) for at in range(0, chans, LANES)]


def stats_kernel(
    place_ref, conv_hbm, grad_hbm, weight_hbm, stats_ref, conv_ref, grad_ref, weight_ref,
    conv_sem, grad_sem, weight_sem,
):
    loads = [
        pltpu.make_async_copy(conv_hbm, conv_ref, conv_sem),
        pltpu.make_async_copy(grad_hbm, grad_ref, grad_sem),
        pltpu.make_async_copy(weight_hbm, weight_ref, weight_sem),
    ]
    for load in loads:
        load.start()
    loads[0].wait()
    rows, chans = conv_ref.shape
    step = 128
    left = left_half(step)
    for begin in range(0, rows, step):
        at = slice(begin, begin + step)
        total = jnp.sum(
            sum(conv_ref[at, c].astype(F32) for c in tiles(chans)), axis=1, keepdims=True
        )
        mean = jnp.broadcast_to(total * (1.0 / chans), (step, LANES))
        spread = 0.0
        for c in tiles(chans):
            off = conv_ref[at, c].astype(F32) - mean
            spread = spread + off * off
        stats_ref[at, :] = jnp.where(left, total, jnp.sum(spread, axis=1, keepdims=True))
    for load in loads[1:]:
        load.wait()


def turn_kernel(place_ref, grad_ref, turned_ref):
    _, width = grad_ref.shape
    piece = width // place_ref.shape[0]
    span = LANES
    each = span // piece

    def body(b, carry):
        columns = pl.ds(pl.multiple_of(b * span, span), span)
        turned = grad_ref[:, columns].T
        for p in range(each):
            to = place_ref[b * each + p]
            turned_ref[pl.ds(pl.multiple_of(to, piece), piece), :] = turned[
                p * piece : (p + 1) * piece, :
            ]
        return carry

    lax.fori_loop(0, width // span, body, 0, unroll=4)


def matmul_kernel(grad_ref, weight_ref, act_grad_ref):
    act_grad_ref[...] = jnp.dot(grad_ref[...], weight_ref[...], preferred_element_type=F32)


def active_kernel(
    conv_ref, own_ref, peer_ref, gain_ref, shift_ref,
    active_ref, normed_ref, deriv_ref, inv_ref, center_ref,
):
    rows, chans = conv_ref.shape
    wide = 128
    for begin in range(0, rows, wide):
        at = slice(begin, begin + wide)
        sum_a, dev_a = both(own_ref[at, :])
        sum_b, dev_b = both(peer_ref[at, :])
        apart = (sum_a - sum_b) * (1.0 / chans)
        variance = (dev_a + dev_b + apart * apart * (0.5 * chans)) * (0.5 / chans)
        center_ref[at, :] = (sum_a + sum_b) * (0.5 / chans)
        inv_ref[at, :] = lax.rsqrt(variance + EPS)
    step = 32

    def body(i, carry):
        at = pl.ds(pl.multiple_of(i * step, step), step)
        center, inv = center_ref[at, :], inv_ref[at, :]
        for c in tiles(chans):
            gain, shift = gain_ref[c].reshape(1, LANES), shift_ref[c].reshape(1, LANES)
            normed = (conv_ref[at, c].astype(F32) - center) * inv
            shifted = normed * gain + shift
            sig = jax.nn.sigmoid(shifted)
            active = shifted * sig
            active_ref[at, c] = active.astype(BF16)
            normed_ref[at, c] = normed
            deriv_ref[at, c] = sig + active * (1.0 - sig)
        return carry

    lax.fori_loop(0, rows // step, body, 0)


def middle_kernel(
    act_grad_ref, normed_ref, deriv_ref, inv_ref, gain_ref, lifted_ref, sums_ref, params_ref,
    total_ref, dot_ref,
):
    rows, chans = act_grad_ref.shape
    wide = 128
    step = 32

    def fold(x):
        return jnp.sum(x.reshape(step // 8, 8, LANES), axis=0)

    def body(i, carry):
        out = []
        at = pl.ds(pl.multiple_of(i * step, step), step)
        inv = inv_ref[at, :]
        total, dot = 0.0, 0.0
        for k, c in enumerate(tiles(chans)):
            normed = normed_ref[at, c]
            norm_grad = act_grad_ref[at, c] * deriv_ref[at, c]
            along = norm_grad * normed
            gain = gain_ref[c].reshape(1, LANES)
            scaled = norm_grad * gain
            lifted_ref[at, c] = scaled * inv
            total = total + scaled
            dot = dot + along * gain
            out.append(carry[2 * k] + fold(along))
            out.append(carry[2 * k + 1] + fold(norm_grad))
        total_ref[at, :] = total
        dot_ref[at, :] = dot
        return tuple(out)

    zero = jnp.zeros((8, LANES), F32)
    folded = lax.fori_loop(0, rows // step, body, (zero,) * (2 * len(tiles(chans))))
    for k, c in enumerate(tiles(chans)):
        params_ref[0:1, c] = jnp.sum(folded[2 * k], axis=0, keepdims=True)
        params_ref[1:2, c] = jnp.sum(folded[2 * k + 1], axis=0, keepdims=True)
    left = left_half(wide)
    for begin in range(0, rows, wide):
        at = slice(begin, begin + wide)
        sums_ref[at, :] = jnp.where(
            left,
            jnp.sum(total_ref[at, :], axis=1, keepdims=True),
            jnp.sum(dot_ref[at, :], axis=1, keepdims=True),
        )


def project_kernel(which, turned_ref, active_ref, *out_refs):
    rows = out_refs[0].shape[0]
    for k, out_ref in zip(which, out_refs):
        out_ref[...] = jnp.dot(
            turned_ref[k * rows : (k + 1) * rows, :], active_ref[...], preferred_element_type=F32
        ).astype(BF16)


def head_kernel(
    lifted_ref, normed_ref, inv_ref, sums_ref, sums_peer_ref, mean_ref, slope_ref, head_ref
):
    rows, chans = lifted_ref.shape
    wide = 128
    for begin in range(0, rows, wide):
        at = slice(begin, begin + wide)
        total, dot = both(sums_ref[at, :] + sums_peer_ref[at, :])
        scale = inv_ref[at, :] * (0.5 / chans)
        mean_ref[at, :] = total * scale
        slope_ref[at, :] = dot * scale
    at = slice(0, head_ref.shape[0])
    for c in tiles(chans):
        head_ref[at, c] = (
            lifted_ref[at, c] - mean_ref[at, :] - normed_ref[at, c] * slope_ref[at, :]
        ).astype(BF16)


def fill_heights(heights, lanes, lifted_ref, normed_ref, mean_ref, slope_ref, halo_ref):
    rows = lifted_ref.shape[0]
    tail = halo_ref.shape[0]
    heights[0:rows, :] = (
        lifted_ref[:, lanes] - mean_ref[...] - normed_ref[:, lanes] * slope_ref[...]
    )
    heights[rows : rows + tail, :] = halo_ref[:, lanes].astype(F32)


def strips(body, begin, end):
    def step(i, carry):
        body(i * LANES)
        return carry

    lax.fori_loop(begin // LANES, end // LANES, step, 0)


def lanes_at(at):
    return pl.ds(pl.multiple_of(at, LANES), LANES)


GROUP = 8


def taps_kernel(
    value_ref, gate_ref, lifted_ref, normed_ref, mean_ref, slope_ref, halo_ref, params_ref,
    out_ref, heights, gated, rows_ref,
):
    rows, chans = value_ref.shape
    taps = halo_ref.shape[0] - 1
    reach = taps - 1
    step = 8 * GROUP

    def one(lanes):
        fill_heights(heights, lanes, lifted_ref, normed_ref, mean_ref, slope_ref, halo_ref)
        sig = jax.nn.sigmoid(gate_ref[:, lanes].astype(F32))
        gated[...] = (value_ref[:, lanes].astype(F32) * sig).astype(BF16).astype(F32)

        def body(i, sums):
            at = pl.multiple_of(i * step, step)
            held = [gated[pl.ds(at + 8 * b, 8), :] for b in range(GROUP)]
            out = list(sums)
            for s in range(8):
                overs = range(s, taps, 8)
                there = [
                    heights[pl.ds(at + (8 * m + s), 8), :] for m in range(GROUP + len(overs) - 1)
                ]
                for q, over in enumerate(overs):
                    j = reach - over
                    products = [held[b] * there[b + q] for b in range(GROUP)]
                    while len(products) > 1:
                        products = [a + b for a, b in zip(products[::2], products[1::2])]
                    out[j] = out[j] + products[0]
            return tuple(out)

        zero = jnp.zeros((8, LANES), F32)
        sums = lax.fori_loop(0, rows // step, body, (zero,) * taps)
        for j in range(taps):
            rows_ref[j : j + 1, :] = jnp.sum(sums[j], axis=0, keepdims=True)
        rows_ref[taps : taps + 2, :] = params_ref[:, lanes]
        rows_ref[taps + 2 :, :] = jnp.zeros((rows_ref.shape[0] - taps - 2, LANES), F32)
        out_ref[:, lanes] = rows_ref[...].astype(BF16)

    strips(lambda at: one(lanes_at(at)), 0, chans)


def spread_kernel(
    begin, value_ref, gate_ref, lifted_ref, normed_ref, mean_ref, slope_ref, halo_ref, taps_ref, *refs
):
    grad_value_ref, grad_gate_ref, heights, spread = refs[-4:]
    rows = value_ref.shape[0]
    taps = taps_ref.shape[0]
    reach = taps - 1
    step = 8 * GROUP

    def one(at_lane):
        lanes, there_lanes = lanes_at(at_lane), lanes_at(at_lane - begin)
        fill_heights(heights, lanes, lifted_ref, normed_ref, mean_ref, slope_ref, halo_ref)
        weights = taps_ref[:, lanes].astype(F32)
        for j in range(taps):
            spread[j] = jnp.broadcast_to(weights[j : j + 1, :], (8, LANES))

        def body(i, carry):
            at = pl.multiple_of(i * step, step)
            total = [None] * GROUP
            for s in range(8):
                overs = range(s, taps, 8)
                there = [
                    heights[pl.ds(at + (8 * m + s), 8), :] for m in range(GROUP + len(overs) - 1)
                ]
                for q, over in enumerate(overs):
                    weight = spread[reach - over]
                    for b in range(GROUP):
                        term = weight * there[b + q]
                        total[b] = term if total[b] is None else total[b] + term
            here = pl.ds(at, step)
            gated_grad = jnp.concatenate(total, axis=0)
            sig = jax.nn.sigmoid(gate_ref[here, lanes].astype(F32))
            grad_value = gated_grad * sig
            grad_value_ref[here, there_lanes] = grad_value.astype(BF16)
            grad_gate_ref[here, there_lanes] = (
                grad_value * value_ref[here, lanes].astype(F32) * (1.0 - sig)
            ).astype(BF16)
            return carry

        lax.fori_loop(0, rows // step, body, 0)

    strips(one, begin, begin + grad_value_ref.shape[1])


def added(refs, at=slice(None)):
    return functools.reduce(lambda a, b: a + b, [r[at, :].astype(F32) for r in refs])


def second_kernel(n, *refs):
    landed, small, outs = refs[:n], refs[n : 2 * n], refs[2 * n :]
    rows = landed[0].shape[0] // n
    more = added(small).astype(BF16)
    for k, out in enumerate(outs):
        out[0:rows, :] = added(landed, slice(k * rows, (k + 1) * rows)).astype(BF16)
        out[rows:, :] = more


def third_kernel(*refs):
    landed, (keep_ref, send_ref) = refs[:-2], refs[-2:]
    rows = keep_ref.shape[0]
    keep_ref[...] = added(landed, slice(0, rows))
    send_ref[...] = added(landed, slice(rows, None)).astype(BF16)


def fourth_kernel(keep_ref, sent_ref, came_ref, *outs):
    rows = keep_ref.shape[0]
    own = rows // len(outs)
    small = added((sent_ref, came_ref), slice(rows, None)).astype(BF16)
    for k, out in enumerate(outs):
        at = slice(k * own, (k + 1) * own)
        out[0:own, :] = added((keep_ref, came_ref), at).astype(out.dtype)
        out[own:, :] = small.astype(out.dtype)


def last_kernel(taps, *refs):
    landed, (project_ref, taps_ref, gain_ref, shift_ref) = refs[:-4], refs[-4:]
    own = project_ref.shape[0]
    total = added(landed)
    project_ref[...] = total[:own, :]
    taps_ref[...] = total[own : own + taps, :]
    gain_ref[...] = total[own + taps, :]
    shift_ref[...] = total[own + taps + 1, :]


def local(conv_value, conv_gate, conv_out, conv_taps, norm_gain, norm_shift, proj_weight, out_grad):
    rows, chans = conv_value.shape
    width = out_grad.shape[1]
    taps = conv_taps.shape[0]
    nz, n, _, cores = (lax.axis_size(a) for a in ALL)
    tail = taps + 1
    extra = -(-(taps + 2) // 8) * 8
    own = width // (nz * n * n)

    z, y, x, core = (lax.axis_index(a) for a in ALL)
    group = lax.iota(jnp.int32, nz * n * n)
    away_y, away_x = (group // n + n - y) % n, (group + n - x) % n
    to_z = group // (n * n)
    away_z = (to_z + nz - z) % nz
    odd = (to_z + z) % 2
    slot_z = odd * (nz // 2) + jnp.where(odd == 1, (to_z + nz - (z ^ 1)) % nz, away_z) // 2
    ahead = jnp.where(core == 0, away_x, away_y) * n + jnp.where(core == 0, away_y, away_x)
    place = (ahead * nz + slot_z) * own

    places = [
        (z, y, x, c) for z in range(nz) for y in range(n) for x in range(n) for c in range(cores)
    ]

    def index(z, y, x, c):
        return ((z * n + y) * n + x) * cores + c

    def hop(array, k, stage):
        def to(z, y, x, c):
            if (c == 0) == (stage == 1):
                return index(z, y, (x + k) % n, c)
            return index(z, (y + k) % n, x, c)

        return lax.ppermute(array, ALL, [(index(*at), to(*at)) for at in places])

    def hop_z(array, k):
        return lax.ppermute(array, "sp_0", [(i, (i + k) % nz) for i in range(nz)])

    def swap_z(array):
        return lax.ppermute(array, "sp_0", [(i, i ^ 1) for i in range(nz)])

    def other_core(array):
        return lax.ppermute(array, "tp", [(0, 1), (1, 0)])

    def previous(array):
        return lax.ppermute(array, SP, [(i, i - 1) for i in range(1, nz * n * n)])

    stats, height, grads, weights = call(
        stats_kernel,
        (
            shape((rows, LANES), F32), shape(conv_out.shape, BF16),
            shape(out_grad.shape, BF16), shape(proj_weight.shape, BF16),
        ),
        place, *(pltpu.with_memory_space_constraint(a, pltpu.HBM) for a in (conv_out, out_grad, proj_weight)),
        flops=rows * chans * 100,
        scratch=[pltpu.SemaphoreType.DMA] * 3,
        specs=[pl.BlockSpec(memory_space=pltpu.SMEM)] + [pl.BlockSpec(memory_space=pltpu.HBM)] * 3,
    )
    stats_peer = other_core(stats)
    (turned,) = call(
        turn_kernel,
        (shape((width, rows), BF16),),
        place, grads,
        flops=rows * width * chans,
        specs=[pl.BlockSpec(memory_space=pltpu.SMEM)] + vmem(1),
    )
    active, normed, deriv, inv = call(
        active_kernel,
        (
            shape((rows, chans), BF16), shape((rows, chans), F32), shape((rows, chans), F32),
            shape((rows, LANES), F32),
        ),
        height, stats, stats_peer, norm_gain, norm_shift,
        flops=rows * chans * 1000,
        scratch=[pltpu.VMEM((rows, LANES), F32)],
    )

    def project(*which):
        return call(
            functools.partial(project_kernel, which),
            (shape((width // n, chans), BF16),) * len(which),
            turned, active,
            flops=2 * rows * width * chans * len(which) // n,
        )

    blocks = {}
    blocks.update(zip((1,), project(1)))
    (act_grad,) = call(
        matmul_kernel,
        (shape((rows, chans), F32),),
        grads, weights,
        flops=2 * rows * width * chans,
    )
    lifted, sums, params = call(
        middle_kernel,
        (shape((rows, chans), F32), shape((rows, LANES), F32), shape((2, chans), F32)),
        act_grad, normed, deriv, inv, norm_gain,
        flops=rows * chans * 1000,
        scratch=[pltpu.VMEM((rows, LANES), F32)] * 2,
    )
    sums_peer = other_core(sums)
    blocks.update(zip((2, 3, 0), project(2, 3, 0)))
    mean, slope, head = call(
        head_kernel,
        (shape((rows, LANES), F32), shape((rows, LANES), F32), shape((tail, chans), BF16)),
        lifted, normed, inv, sums, sums_peer,
        flops=rows * chans * 10,
    )
    halo = previous(head)
    landed = [blocks[0], hop(blocks[1], 1, 1)]
    landed.append(hop(blocks[2], 2, 1))
    landed.append(hop(blocks[3], 3, 1))
    heights = (lifted, normed, mean, slope, halo)
    (small,) = call(
        taps_kernel,
        (shape((extra, chans), BF16),),
        conv_value, conv_gate, *heights, params,
        flops=taps * rows * chans * 40,
        scratch=[pltpu.VMEM((rows + tail, LANES), F32), pltpu.VMEM((rows, LANES), F32),
            pltpu.VMEM((extra, LANES), F32),
        ],
    )

    def spread_part(part, before):
        half = chans // 2
        operands = (conv_value, conv_gate, *heights, conv_taps)
        block = pl.BlockSpec((rows, half), lambda i: (0, part))
        return pl.pallas_call(
            functools.partial(spread_kernel, part * half),
            grid=(1,),
            out_shape=(shape((rows, chans), BF16),) * 2,
            in_specs=vmem(len(operands)) + [pl.BlockSpec(memory_space=pl.ANY)] * len(before),
            out_specs=(block, block),
            input_output_aliases={len(operands) + k: k for k in range(len(before))},
            scratch_shapes=[
                pltpu.VMEM((rows + tail, LANES), F32), pltpu.VMEM((taps, 8, LANES), F32),
            ],
            cost_estimate=pl.CostEstimate(
                flops=taps * rows * chans * 20, bytes_accessed=rows * chans * 10, transcendentals=0
            ),
            compiler_params=pltpu.CompilerParams(vmem_limit_bytes=8 * MIB),
            name="spread",
        )(*operands, *before)

    halves = spread_part(0, ())
    grad_value, grad_gate = spread_part(1, halves)
    smalls = [small] + [hop(small, k, 1) for k in range(1, n)]
    part = width // (n * n)
    second = call(
        functools.partial(second_kernel, n),
        (shape((part + extra, chans), BF16),) * n,
        *landed, *smalls,
        flops=width * chans * 100,
    )
    then = [second[0]] + [hop(second[k], k, 2) for k in range(1, n)]
    keep, send = call(
        third_kernel,
        (shape((part // 2, chans), F32), shape((part // 2 + extra, chans), BF16)),
        *then,
        flops=width * chans * 10,
    )
    came = swap_z(send)
    fourth = call(
        fourth_kernel,
        (shape((own + extra, chans), F32),) + (shape((own + extra, chans), BF16),) * (nz // 2 - 1),
        keep, send, came,
        flops=width * chans * 10,
    )
    fars = [fourth[0]] + [hop_z(fourth[k], 2 * k) for k in range(1, nz // 2)]
    grad_proj, grad_taps, grad_gain, grad_shift = call(
        functools.partial(last_kernel, taps),
        (shape((own, chans), F32), shape((taps, chans), F32), shape((chans,), F32), shape((chans,), F32)),
        *fars,
        flops=width * chans * 10,
    )
    return grad_value, grad_gate, grad_taps, grad_gain, grad_shift, grad_proj


def solution(mesh):
    split = Mesh(mesh.devices.reshape(8, 4, 4, mesh.shape["tp"]), ALL)
    placed = (
        P(SP, "tp"),
        P(SP, "tp"),
        P(SP, "tp"),
        P(None, "tp"),
        P("tp"),
        P("tp"),
        P(None, "tp"),
        P(SP, None),
    )
    return jax.shard_map(
        local,
        mesh=split,
        in_specs=placed,
        out_specs=(P(SP, "tp"), P(SP, "tp"), P(None, "tp"), P("tp"), P("tp"), P(SP, "tp")),
        check_vma=False,
    )
```

```python
import functools

import jax
import jax.numpy as jnp
from jax import lax
from jax.experimental import pallas as pl
from jax.experimental.pallas import tpu as pltpu
from jax.sharding import Mesh
from jax.sharding import PartitionSpec as P


SP = ("sp_0", "sp_1", "sp_2")
ALL = SP + ("tp",)
EPS = 1e-05
F32 = jnp.float32
BF16 = jnp.bfloat16
LANES = 128
MIB = 1024 * 1024


def vmem(count):
    return [pl.BlockSpec(memory_space=pltpu.VMEM)] * count


def call(kernel, outs, *args, flops, scratch=(), specs=None, limit=8):
    moved = sum(a.size * a.dtype.itemsize for a in args) + sum(
        o.size * o.dtype.itemsize for o in outs
    )
    return pl.pallas_call(
        kernel,
        out_shape=outs,
        in_specs=specs or vmem(len(args)),
        out_specs=vmem(len(outs)),
        scratch_shapes=list(scratch),
        cost_estimate=pl.CostEstimate(flops=flops, bytes_accessed=moved, transcendentals=0),
        compiler_params=pltpu.CompilerParams(vmem_limit_bytes=limit * MIB),
    )(*args)


def shape(dims, dtype):
    return jax.ShapeDtypeStruct(dims, dtype)


def left_half(rows):
    return lax.broadcasted_iota(jnp.int32, (rows, LANES), 1) < LANES // 2


def both(packed):
    left = left_half(packed.shape[0])
    turned = pltpu.roll(packed, LANES // 2, 1)
    return jnp.where(left, packed, turned), jnp.where(left, turned, packed)


def tiles(chans):
    return [slice(at, at + LANES) for at in range(0, chans, LANES)]


def stats_kernel(
    place_ref, conv_hbm, grad_hbm, weight_hbm, stats_ref, conv_ref, grad_ref, weight_ref,
    conv_sem, grad_sem, weight_sem,
):
    loads = [
        pltpu.make_async_copy(conv_hbm, conv_ref, conv_sem),
        pltpu.make_async_copy(grad_hbm, grad_ref, grad_sem),
        pltpu.make_async_copy(weight_hbm, weight_ref, weight_sem),
    ]
    for load in loads:
        load.start()
    loads[0].wait()
    rows, chans = conv_ref.shape
    step = 128
    left = left_half(step)
    for begin in range(0, rows, step):
        at = slice(begin, begin + step)
        total = jnp.sum(
            sum(conv_ref[at, c].astype(F32) for c in tiles(chans)), axis=1, keepdims=True
        )
        mean = jnp.broadcast_to(total * (1.0 / chans), (step, LANES))
        spread = 0.0
        for c in tiles(chans):
            off = conv_ref[at, c].astype(F32) - mean
            spread = spread + off * off
        stats_ref[at, :] = jnp.where(left, total, jnp.sum(spread, axis=1, keepdims=True))
    for load in loads[1:]:
        load.wait()


def turn_kernel(place_ref, grad_ref, turned_ref):
    _, width = grad_ref.shape
    piece = width // place_ref.shape[0]
    span = LANES
    each = span // piece

    def body(b, carry):
        columns = pl.ds(pl.multiple_of(b * span, span), span)
        turned = grad_ref[:, columns].T
        for p in range(each):
            to = place_ref[b * each + p]
            turned_ref[pl.ds(pl.multiple_of(to, piece), piece), :] = turned[
                p * piece : (p + 1) * piece, :
            ]
        return carry

    lax.fori_loop(0, width // span, body, 0, unroll=4)


def matmul_kernel(grad_ref, weight_ref, act_grad_ref):
    act_grad_ref[...] = jnp.dot(grad_ref[...], weight_ref[...], preferred_element_type=F32)


def active_kernel(
    conv_ref, own_ref, peer_ref, gain_ref, shift_ref,
    active_ref, normed_ref, deriv_ref, inv_ref, center_ref,
):
    rows, chans = conv_ref.shape
    wide = 128
    for begin in range(0, rows, wide):
        at = slice(begin, begin + wide)
        sum_a, dev_a = both(own_ref[at, :])
        sum_b, dev_b = both(peer_ref[at, :])
        apart = (sum_a - sum_b) * (1.0 / chans)
        variance = (dev_a + dev_b + apart * apart * (0.5 * chans)) * (0.5 / chans)
        center_ref[at, :] = (sum_a + sum_b) * (0.5 / chans)
        inv_ref[at, :] = lax.rsqrt(variance + EPS)
    step = 32

    def body(i, carry):
        at = pl.ds(pl.multiple_of(i * step, step), step)
        center, inv = center_ref[at, :], inv_ref[at, :]
        for c in tiles(chans):
            gain, shift = gain_ref[c].reshape(1, LANES), shift_ref[c].reshape(1, LANES)
            normed = (conv_ref[at, c].astype(F32) - center) * inv
            shifted = normed * gain + shift
            sig = jax.nn.sigmoid(shifted)
            active = shifted * sig
            active_ref[at, c] = active.astype(BF16)
            normed_ref[at, c] = normed
            deriv_ref[at, c] = sig + active * (1.0 - sig)
        return carry

    lax.fori_loop(0, rows // step, body, 0)


def middle_kernel(
    act_grad_ref, normed_ref, deriv_ref, inv_ref, gain_ref, lifted_ref, sums_ref, params_ref,
    total_ref, dot_ref,
):
    rows, chans = act_grad_ref.shape
    wide = 128
    step = 32

    def fold(x):
        return jnp.sum(x.reshape(step // 8, 8, LANES), axis=0)

    def body(i, carry):
        out = []
        at = pl.ds(pl.multiple_of(i * step, step), step)
        inv = inv_ref[at, :]
        total, dot = 0.0, 0.0
        for k, c in enumerate(tiles(chans)):
            normed = normed_ref[at, c]
            norm_grad = act_grad_ref[at, c] * deriv_ref[at, c]
            along = norm_grad * normed
            gain = gain_ref[c].reshape(1, LANES)
            scaled = norm_grad * gain
            lifted_ref[at, c] = scaled * inv
            total = total + scaled
            dot = dot + along * gain
            out.append(carry[2 * k] + fold(along))
            out.append(carry[2 * k + 1] + fold(norm_grad))
        total_ref[at, :] = total
        dot_ref[at, :] = dot
        return tuple(out)

    zero = jnp.zeros((8, LANES), F32)
    folded = lax.fori_loop(0, rows // step, body, (zero,) * (2 * len(tiles(chans))))
    for k, c in enumerate(tiles(chans)):
        params_ref[0:1, c] = jnp.sum(folded[2 * k], axis=0, keepdims=True)
        params_ref[1:2, c] = jnp.sum(folded[2 * k + 1], axis=0, keepdims=True)
    left = left_half(wide)
    for begin in range(0, rows, wide):
        at = slice(begin, begin + wide)
        sums_ref[at, :] = jnp.where(
            left,
            jnp.sum(total_ref[at, :], axis=1, keepdims=True),
            jnp.sum(dot_ref[at, :], axis=1, keepdims=True),
        )


def project_kernel(which, turned_ref, active_ref, *out_refs):
    rows = out_refs[0].shape[0]
    for k, out_ref in zip(which, out_refs):
        out_ref[...] = jnp.dot(
            turned_ref[k * rows : (k + 1) * rows, :], active_ref[...], preferred_element_type=F32
        ).astype(BF16)


def head_kernel(
    lifted_ref, normed_ref, inv_ref, sums_ref, sums_peer_ref, mean_ref, slope_ref, head_ref
):
    rows, chans = lifted_ref.shape
    wide = 128
    for begin in range(0, rows, wide):
        at = slice(begin, begin + wide)
        total, dot = both(sums_ref[at, :] + sums_peer_ref[at, :])
        scale = inv_ref[at, :] * (0.5 / chans)
        mean_ref[at, :] = total * scale
        slope_ref[at, :] = dot * scale
    at = slice(0, head_ref.shape[0])
    for c in tiles(chans):
        head_ref[at, c] = (
            lifted_ref[at, c] - mean_ref[at, :] - normed_ref[at, c] * slope_ref[at, :]
        ).astype(BF16)


def fill_heights(heights, lanes, lifted_ref, normed_ref, mean_ref, slope_ref, halo_ref):
    rows = lifted_ref.shape[0]
    tail = halo_ref.shape[0]
    heights[0:rows, :] = (
        lifted_ref[:, lanes] - mean_ref[...] - normed_ref[:, lanes] * slope_ref[...]
    )
    heights[rows : rows + tail, :] = halo_ref[:, lanes].astype(F32)


def strips(body, begin, end):
    def step(i, carry):
        body(i * LANES)
        return carry

    lax.fori_loop(begin // LANES, end // LANES, step, 0)


def lanes_at(at):
    return pl.ds(pl.multiple_of(at, LANES), LANES)


GROUP = 8


def taps_kernel(
    value_ref, gate_ref, lifted_ref, normed_ref, mean_ref, slope_ref, halo_ref, params_ref,
    out_ref, heights, gated, rows_ref,
):
    rows, chans = value_ref.shape
    taps = halo_ref.shape[0] - 1
    reach = taps - 1
    step = 8 * GROUP

    def one(lanes):
        fill_heights(heights, lanes, lifted_ref, normed_ref, mean_ref, slope_ref, halo_ref)
        sig = jax.nn.sigmoid(gate_ref[:, lanes].astype(F32))
        gated[...] = (value_ref[:, lanes].astype(F32) * sig).astype(BF16).astype(F32)

        def body(i, sums):
            at = pl.multiple_of(i * step, step)
            held = [gated[pl.ds(at + 8 * b, 8), :] for b in range(GROUP)]
            out = list(sums)
            for s in range(8):
                overs = range(s, taps, 8)
                there = [
                    heights[pl.ds(at + (8 * m + s), 8), :] for m in range(GROUP + len(overs) - 1)
                ]
                for q, over in enumerate(overs):
                    j = reach - over
                    products = [held[b] * there[b + q] for b in range(GROUP)]
                    while len(products) > 1:
                        products = [a + b for a, b in zip(products[::2], products[1::2])]
                    out[j] = out[j] + products[0]
            return tuple(out)

        zero = jnp.zeros((8, LANES), F32)
        sums = lax.fori_loop(0, rows // step, body, (zero,) * taps)
        for j in range(taps):
            rows_ref[j : j + 1, :] = jnp.sum(sums[j], axis=0, keepdims=True)
        rows_ref[taps : taps + 2, :] = params_ref[:, lanes]
        rows_ref[taps + 2 :, :] = jnp.zeros((rows_ref.shape[0] - taps - 2, LANES), F32)
        out_ref[:, lanes] = rows_ref[...].astype(BF16)

    strips(lambda at: one(lanes_at(at)), 0, chans)


def spread_kernel(
    begin, value_ref, gate_ref, lifted_ref, normed_ref, mean_ref, slope_ref, halo_ref, taps_ref, *refs
):
    grad_value_ref, grad_gate_ref, heights, spread = refs[-4:]
    rows = value_ref.shape[0]
    taps = taps_ref.shape[0]
    reach = taps - 1
    step = 8 * GROUP

    def one(at_lane):
        lanes, there_lanes = lanes_at(at_lane), lanes_at(at_lane - begin)
        fill_heights(heights, lanes, lifted_ref, normed_ref, mean_ref, slope_ref, halo_ref)
        weights = taps_ref[:, lanes].astype(F32)
        for j in range(taps):
            spread[j] = jnp.broadcast_to(weights[j : j + 1, :], (8, LANES))

        def body(i, carry):
            at = pl.multiple_of(i * step, step)
            total = [None] * GROUP
            for s in range(8):
                overs = range(s, taps, 8)
                there = [
                    heights[pl.ds(at + (8 * m + s), 8), :] for m in range(GROUP + len(overs) - 1)
                ]
                for q, over in enumerate(overs):
                    weight = spread[reach - over]
                    for b in range(GROUP):
                        term = weight * there[b + q]
                        total[b] = term if total[b] is None else total[b] + term
            here = pl.ds(at, step)
            gated_grad = jnp.concatenate(total, axis=0)
            sig = jax.nn.sigmoid(gate_ref[here, lanes].astype(F32))
            grad_value = gated_grad * sig
            grad_value_ref[here, there_lanes] = grad_value.astype(BF16)
            grad_gate_ref[here, there_lanes] = (
                grad_value * value_ref[here, lanes].astype(F32) * (1.0 - sig)
            ).astype(BF16)
            return carry

        lax.fori_loop(0, rows // step, body, 0)

    strips(one, begin, begin + grad_value_ref.shape[1])


def added(refs, at=slice(None)):
    return functools.reduce(lambda a, b: a + b, [r[at, :].astype(F32) for r in refs])


def second_kernel(n, *refs):
    landed, small, outs = refs[:n], refs[n : 2 * n], refs[2 * n :]
    rows = landed[0].shape[0] // n
    more = added(small).astype(BF16)
    for k, out in enumerate(outs):
        out[0:rows, :] = added(landed, slice(k * rows, (k + 1) * rows)).astype(BF16)
        out[rows:, :] = more


def third_kernel(*refs):
    landed, (keep_ref, send_ref) = refs[:-2], refs[-2:]
    rows = keep_ref.shape[0]
    keep_ref[...] = added(landed, slice(0, rows))
    send_ref[...] = added(landed, slice(rows, None)).astype(BF16)


def fourth_kernel(keep_ref, sent_ref, came_ref, *outs):
    rows = keep_ref.shape[0]
    own = rows // len(outs)
    small = added((sent_ref, came_ref), slice(rows, None)).astype(BF16)
    for k, out in enumerate(outs):
        at = slice(k * own, (k + 1) * own)
        out[0:own, :] = added((keep_ref, came_ref), at).astype(out.dtype)
        out[own:, :] = small.astype(out.dtype)


def last_kernel(taps, *refs):
    landed, (project_ref, taps_ref, gain_ref, shift_ref) = refs[:-4], refs[-4:]
    own = project_ref.shape[0]
    total = added(landed)
    project_ref[...] = total[:own, :]
    taps_ref[...] = total[own : own + taps, :]
    gain_ref[...] = total[own + taps, :]
    shift_ref[...] = total[own + taps + 1, :]


def local(conv_value, conv_gate, conv_out, conv_taps, norm_gain, norm_shift, proj_weight, out_grad):
    rows, chans = conv_value.shape
    width = out_grad.shape[1]
    taps = conv_taps.shape[0]
    nz, n, _, cores = (lax.axis_size(a) for a in ALL)
    tail = taps + 1
    extra = -(-(taps + 2) // 8) * 8
    own = width // (nz * n * n)

    z, y, x, core = (lax.axis_index(a) for a in ALL)
    group = lax.iota(jnp.int32, nz * n * n)
    off_y, off_x = (group // n) % n ^ y, group % n ^ x

    def pair_bits(off):
        first = ((off == 1) | (off == 2)).astype(jnp.int32)
        second = (off >= 2).astype(jnp.int32)
        return jnp.where(core == 0, first, second), jnp.where(core == 0, second, first)

    (now_y, then_y), (now_x, then_x) = pair_bits(off_y), pair_bits(off_x)
    to_z = group // (n * n)
    odd = (to_z + z) % 2
    slot_z = odd * (nz // 2) + (to_z + nz - (z ^ odd)) % nz // 2
    ahead = (2 * now_y + now_x) * n + 2 * then_y + then_x
    place = (ahead * nz + slot_z) * own

    places = [
        (z, y, x, c) for z in range(nz) for y in range(n) for x in range(n) for c in range(cores)
    ]

    def index(z, y, x, c):
        return ((z * n + y) * n + x) * cores + c

    def hop(array, k, stage):
        def to(z, y, x, c):
            step = 1 if (c == 0) == (stage == 1) else 3
            return index(z, y ^ k // 2 * step, x ^ k % 2 * step, c)

        return lax.ppermute(array, ALL, [(index(*at), to(*at)) for at in places])

    def hop_z(array, k):
        return lax.ppermute(array, "sp_0", [(i, (i + k) % nz) for i in range(nz)])

    def swap_z(array):
        return lax.ppermute(array, "sp_0", [(i, i ^ 1) for i in range(nz)])

    def other_core(array):
        return lax.ppermute(array, "tp", [(0, 1), (1, 0)])

    def previous(array):
        return lax.ppermute(array, SP, [(i, i - 1) for i in range(1, nz * n * n)])

    stats, height, grads, weights = call(
        stats_kernel,
        (
            shape((rows, LANES), F32), shape(conv_out.shape, BF16),
            shape(out_grad.shape, BF16), shape(proj_weight.shape, BF16),
        ),
        place, *(pltpu.with_memory_space_constraint(a, pltpu.HBM) for a in (conv_out, out_grad, proj_weight)),
        flops=rows * chans * 100,
        scratch=[pltpu.SemaphoreType.DMA] * 3,
        specs=[pl.BlockSpec(memory_space=pltpu.SMEM)] + [pl.BlockSpec(memory_space=pltpu.HBM)] * 3,
    )
    stats_peer = other_core(stats)
    (turned,) = call(
        turn_kernel,
        (shape((width, rows), BF16),),
        place, grads,
        flops=rows * width * chans,
        specs=[pl.BlockSpec(memory_space=pltpu.SMEM)] + vmem(1),
    )
    active, normed, deriv, inv = call(
        active_kernel,
        (
            shape((rows, chans), BF16), shape((rows, chans), F32), shape((rows, chans), F32),
            shape((rows, LANES), F32),
        ),
        height, stats, stats_peer, norm_gain, norm_shift,
        flops=rows * chans * 1000,
        scratch=[pltpu.VMEM((rows, LANES), F32)],
    )

    def project(*which):
        return call(
            functools.partial(project_kernel, which),
            (shape((width // n, chans), BF16),) * len(which),
            turned, active,
            flops=2 * rows * width * chans * len(which) // n,
        )

    blocks = {}
    blocks.update(zip((1, 2), project(1, 2)))
    (act_grad,) = call(
        matmul_kernel,
        (shape((rows, chans), F32),),
        grads, weights,
        flops=2 * rows * width * chans,
    )
    lifted, sums, params = call(
        middle_kernel,
        (shape((rows, chans), F32), shape((rows, LANES), F32), shape((2, chans), F32)),
        act_grad, normed, deriv, inv, norm_gain,
        flops=rows * chans * 1000,
        scratch=[pltpu.VMEM((rows, LANES), F32)] * 2,
    )
    sums_peer = other_core(sums)
    blocks.update(zip((3, 0), project(3, 0)))
    mean, slope, head = call(
        head_kernel,
        (shape((rows, LANES), F32), shape((rows, LANES), F32), shape((tail, chans), BF16)),
        lifted, normed, inv, sums, sums_peer,
        flops=rows * chans * 10,
    )
    halo = previous(head)
    landed = [blocks[0], hop(blocks[1], 1, 1)]
    landed.append(hop(blocks[2], 2, 1))
    landed.append(hop(blocks[3], 3, 1))
    heights = (lifted, normed, mean, slope, halo)
    (small,) = call(
        taps_kernel,
        (shape((extra, chans), BF16),),
        conv_value, conv_gate, *heights, params,
        flops=taps * rows * chans * 40,
        scratch=[pltpu.VMEM((rows + tail, LANES), F32), pltpu.VMEM((rows, LANES), F32),
            pltpu.VMEM((extra, LANES), F32),
        ],
    )

    def spread_part(part, before):
        half = chans // 2
        operands = (conv_value, conv_gate, *heights, conv_taps)
        block = pl.BlockSpec((rows, half), lambda i: (0, part))
        return pl.pallas_call(
            functools.partial(spread_kernel, part * half),
            grid=(1,),
            out_shape=(shape((rows, chans), BF16),) * 2,
            in_specs=vmem(len(operands)) + [pl.BlockSpec(memory_space=pl.ANY)] * len(before),
            out_specs=(block, block),
            input_output_aliases={len(operands) + k: k for k in range(len(before))},
            scratch_shapes=[
                pltpu.VMEM((rows + tail, LANES), F32), pltpu.VMEM((taps, 8, LANES), F32),
            ],
            cost_estimate=pl.CostEstimate(
                flops=taps * rows * chans * 20, bytes_accessed=rows * chans * 10, transcendentals=0
            ),
            compiler_params=pltpu.CompilerParams(vmem_limit_bytes=8 * MIB),
            name="spread",
        )(*operands, *before)

    halves = spread_part(0, ())
    grad_value, grad_gate = spread_part(1, halves)
    smalls = [small] + [hop(small, k, 1) for k in range(1, n)]
    part = width // (n * n)
    second = call(
        functools.partial(second_kernel, n),
        (shape((part + extra, chans), BF16),) * n,
        *landed, *smalls,
        flops=width * chans * 100,
    )
    then = [second[0]] + [hop(second[k], k, 2) for k in range(1, n)]
    keep, send = call(
        third_kernel,
        (shape((part // 2, chans), F32), shape((part // 2 + extra, chans), BF16)),
        *then,
        flops=width * chans * 10,
    )
    came = swap_z(send)
    fourth = call(
        fourth_kernel,
        (shape((own + extra, chans), F32),) + (shape((own + extra, chans), BF16),) * (nz // 2 - 1),
        keep, send, came,
        flops=width * chans * 10,
    )
    fars = [fourth[0]] + [hop_z(fourth[k], 2 * k) for k in range(1, nz // 2)]
    grad_proj, grad_taps, grad_gain, grad_shift = call(
        functools.partial(last_kernel, taps),
        (shape((own, chans), F32), shape((taps, chans), F32), shape((chans,), F32), shape((chans,), F32)),
        *fars,
        flops=width * chans * 10,
    )
    return grad_value, grad_gate, grad_taps, grad_gain, grad_shift, grad_proj


def solution(mesh):
    split = Mesh(mesh.devices.reshape(8, 4, 4, mesh.shape["tp"]), ALL)
    placed = (
        P(SP, "tp"),
        P(SP, "tp"),
        P(SP, "tp"),
        P(None, "tp"),
        P("tp"),
        P("tp"),
        P(None, "tp"),
        P(SP, None),
    )
    return jax.shard_map(
        local,
        mesh=split,
        in_specs=placed,
        out_specs=(P(SP, "tp"), P(SP, "tp"), P(None, "tp"), P("tp"), P("tp"), P(SP, "tp")),
        check_vma=False,
    )
```

```python
import functools

import jax
import jax.numpy as jnp
from jax import lax
from jax.experimental import pallas as pl
from jax.experimental.pallas import tpu as pltpu
from jax.sharding import Mesh
from jax.sharding import PartitionSpec as P


SP = ("sp_0", "sp_1", "sp_2")
ALL = SP + ("tp",)
EPS = 1e-05
F32 = jnp.float32
BF16 = jnp.bfloat16
LANES = 128
MIB = 1024 * 1024


def vmem(count):
    return [pl.BlockSpec(memory_space=pltpu.VMEM)] * count


def call(kernel, outs, *args, flops, scratch=(), specs=None, limit=8):
    moved = sum(a.size * a.dtype.itemsize for a in args) + sum(
        o.size * o.dtype.itemsize for o in outs
    )
    return pl.pallas_call(
        kernel,
        out_shape=outs,
        in_specs=specs or vmem(len(args)),
        out_specs=vmem(len(outs)),
        scratch_shapes=list(scratch),
        cost_estimate=pl.CostEstimate(flops=flops, bytes_accessed=moved, transcendentals=0),
        compiler_params=pltpu.CompilerParams(vmem_limit_bytes=limit * MIB),
    )(*args)


def shape(dims, dtype):
    return jax.ShapeDtypeStruct(dims, dtype)


def left_half(rows):
    return lax.broadcasted_iota(jnp.int32, (rows, LANES), 1) < LANES // 2


def both(packed):
    left = left_half(packed.shape[0])
    turned = pltpu.roll(packed, LANES // 2, 1)
    return jnp.where(left, packed, turned), jnp.where(left, turned, packed)


def tiles(chans):
    return [slice(at, at + LANES) for at in range(0, chans, LANES)]


def stats_kernel(
    place_ref, conv_hbm, grad_hbm, stats_ref, conv_ref, grad_ref, conv_sem, grad_sem
):
    loads = [
        pltpu.make_async_copy(conv_hbm, conv_ref, conv_sem),
        pltpu.make_async_copy(grad_hbm, grad_ref, grad_sem),
    ]
    for load in loads:
        load.start()
    loads[0].wait()
    rows, chans = conv_ref.shape
    step = 128
    left = left_half(step)
    for begin in range(0, rows, step):
        at = slice(begin, begin + step)
        total = jnp.sum(
            sum(conv_ref[at, c].astype(F32) for c in tiles(chans)), axis=1, keepdims=True
        )
        mean = jnp.broadcast_to(total * (1.0 / chans), (step, LANES))
        spread = 0.0
        for c in tiles(chans):
            off = conv_ref[at, c].astype(F32) - mean
            spread = spread + off * off
        stats_ref[at, :] = jnp.where(left, total, jnp.sum(spread, axis=1, keepdims=True))
    loads[1].wait()


def turn_kernel(place_ref, grad_ref, turned_ref):
    _, width = grad_ref.shape
    piece = width // place_ref.shape[0]
    span = LANES
    each = span // piece

    def body(b, carry):
        columns = pl.ds(pl.multiple_of(b * span, span), span)
        turned = grad_ref[:, columns].T
        for p in range(each):
            to = place_ref[b * each + p]
            turned_ref[pl.ds(pl.multiple_of(to, piece), piece), :] = turned[
                p * piece : (p + 1) * piece, :
            ]
        return carry

    lax.fori_loop(0, width // span, body, 0, unroll=4)


def matmul_kernel(grad_ref, weight_ref, act_grad_ref):
    act_grad_ref[...] = jnp.dot(grad_ref[...], weight_ref[...], preferred_element_type=F32)


def active_kernel(
    conv_ref, own_ref, peer_ref, gain_ref, shift_ref,
    active_ref, normed_ref, deriv_ref, inv_ref, center_ref,
):
    rows, chans = conv_ref.shape
    wide = 128
    for begin in range(0, rows, wide):
        at = slice(begin, begin + wide)
        sum_a, dev_a = both(own_ref[at, :])
        sum_b, dev_b = both(peer_ref[at, :])
        apart = (sum_a - sum_b) * (1.0 / chans)
        variance = (dev_a + dev_b + apart * apart * (0.5 * chans)) * (0.5 / chans)
        center_ref[at, :] = (sum_a + sum_b) * (0.5 / chans)
        inv_ref[at, :] = lax.rsqrt(variance + EPS)
    step = 32

    def body(i, carry):
        at = pl.ds(pl.multiple_of(i * step, step), step)
        center, inv = center_ref[at, :], inv_ref[at, :]
        for c in tiles(chans):
            gain, shift = gain_ref[c].reshape(1, LANES), shift_ref[c].reshape(1, LANES)
            normed = (conv_ref[at, c].astype(F32) - center) * inv
            shifted = normed * gain + shift
            sig = jax.nn.sigmoid(shifted)
            active = shifted * sig
            active_ref[at, c] = active.astype(BF16)
            normed_ref[at, c] = normed
            deriv_ref[at, c] = sig + active * (1.0 - sig)
        return carry

    lax.fori_loop(0, rows // step, body, 0)


def middle_kernel(
    act_grad_ref, normed_ref, deriv_ref, inv_ref, gain_ref, lifted_ref, sums_ref, params_ref,
    total_ref, dot_ref,
):
    rows, chans = act_grad_ref.shape
    wide = 128
    step = 32

    def fold(x):
        return jnp.sum(x.reshape(step // 8, 8, LANES), axis=0)

    def body(i, carry):
        out = []
        at = pl.ds(pl.multiple_of(i * step, step), step)
        inv = inv_ref[at, :]
        total, dot = 0.0, 0.0
        for k, c in enumerate(tiles(chans)):
            normed = normed_ref[at, c]
            norm_grad = act_grad_ref[at, c] * deriv_ref[at, c]
            along = norm_grad * normed
            gain = gain_ref[c].reshape(1, LANES)
            scaled = norm_grad * gain
            lifted_ref[at, c] = scaled * inv
            total = total + scaled
            dot = dot + along * gain
            out.append(carry[2 * k] + fold(along))
            out.append(carry[2 * k + 1] + fold(norm_grad))
        total_ref[at, :] = total
        dot_ref[at, :] = dot
        return tuple(out)

    zero = jnp.zeros((8, LANES), F32)
    folded = lax.fori_loop(0, rows // step, body, (zero,) * (2 * len(tiles(chans))))
    for k, c in enumerate(tiles(chans)):
        params_ref[0:1, c] = jnp.sum(folded[2 * k], axis=0, keepdims=True)
        params_ref[1:2, c] = jnp.sum(folded[2 * k + 1], axis=0, keepdims=True)
    left = left_half(wide)
    for begin in range(0, rows, wide):
        at = slice(begin, begin + wide)
        sums_ref[at, :] = jnp.where(
            left,
            jnp.sum(total_ref[at, :], axis=1, keepdims=True),
            jnp.sum(dot_ref[at, :], axis=1, keepdims=True),
        )


def project_kernel(which, turned_ref, active_ref, *out_refs):
    rows = out_refs[0].shape[0]
    for k, out_ref in zip(which, out_refs):
        out_ref[...] = jnp.dot(
            turned_ref[k * rows : (k + 1) * rows, :], active_ref[...], preferred_element_type=F32
        ).astype(BF16)


def head_kernel(
    lifted_ref, normed_ref, inv_ref, sums_ref, sums_peer_ref, mean_ref, slope_ref, head_ref
):
    rows, chans = lifted_ref.shape
    wide = 128
    for begin in range(0, rows, wide):
        at = slice(begin, begin + wide)
        total, dot = both(sums_ref[at, :] + sums_peer_ref[at, :])
        scale = inv_ref[at, :] * (0.5 / chans)
        mean_ref[at, :] = total * scale
        slope_ref[at, :] = dot * scale
    at = slice(0, head_ref.shape[0])
    for c in tiles(chans):
        head_ref[at, c] = (
            lifted_ref[at, c] - mean_ref[at, :] - normed_ref[at, c] * slope_ref[at, :]
        ).astype(BF16)


def fill_heights(heights, lanes, lifted_ref, normed_ref, mean_ref, slope_ref, halo_ref):
    rows = lifted_ref.shape[0]
    tail = halo_ref.shape[0]
    heights[0:rows, :] = (
        lifted_ref[:, lanes] - mean_ref[...] - normed_ref[:, lanes] * slope_ref[...]
    )
    heights[rows : rows + tail, :] = halo_ref[:, lanes].astype(F32)


def strips(body, begin, end):
    def step(i, carry):
        body(i * LANES)
        return carry

    lax.fori_loop(begin // LANES, end // LANES, step, 0)


def lanes_at(at):
    return pl.ds(pl.multiple_of(at, LANES), LANES)


GROUP = 8


def taps_kernel(
    value_ref, gate_ref, lifted_ref, normed_ref, mean_ref, slope_ref, halo_ref, params_ref,
    out_ref, heights, gated, rows_ref,
):
    rows, chans = value_ref.shape
    taps = halo_ref.shape[0] - 1
    reach = taps - 1
    step = 8 * GROUP

    def one(lanes):
        fill_heights(heights, lanes, lifted_ref, normed_ref, mean_ref, slope_ref, halo_ref)
        sig = jax.nn.sigmoid(gate_ref[:, lanes].astype(F32))
        gated[...] = (value_ref[:, lanes].astype(F32) * sig).astype(BF16).astype(F32)

        def body(i, sums):
            at = pl.multiple_of(i * step, step)
            held = [gated[pl.ds(at + 8 * b, 8), :] for b in range(GROUP)]
            out = list(sums)
            for s in range(8):
                overs = range(s, taps, 8)
                there = [
                    heights[pl.ds(at + (8 * m + s), 8), :] for m in range(GROUP + len(overs) - 1)
                ]
                for q, over in enumerate(overs):
                    j = reach - over
                    products = [held[b] * there[b + q] for b in range(GROUP)]
                    while len(products) > 1:
                        products = [a + b for a, b in zip(products[::2], products[1::2])]
                    out[j] = out[j] + products[0]
            return tuple(out)

        zero = jnp.zeros((8, LANES), F32)
        sums = lax.fori_loop(0, rows // step, body, (zero,) * taps)
        for j in range(taps):
            rows_ref[j : j + 1, :] = jnp.sum(sums[j], axis=0, keepdims=True)
        rows_ref[taps : taps + 2, :] = params_ref[:, lanes]
        rows_ref[taps + 2 :, :] = jnp.zeros((rows_ref.shape[0] - taps - 2, LANES), F32)
        out_ref[:, lanes] = rows_ref[...].astype(BF16)

    strips(lambda at: one(lanes_at(at)), 0, chans)


def spread_kernel(
    begin, value_ref, gate_ref, lifted_ref, normed_ref, mean_ref, slope_ref, halo_ref, taps_ref, *refs
):
    grad_value_ref, grad_gate_ref, heights, spread = refs[-4:]
    rows = value_ref.shape[0]
    taps = taps_ref.shape[0]
    reach = taps - 1
    step = 8 * GROUP

    def one(at_lane):
        lanes, there_lanes = lanes_at(at_lane), lanes_at(at_lane - begin)
        fill_heights(heights, lanes, lifted_ref, normed_ref, mean_ref, slope_ref, halo_ref)
        weights = taps_ref[:, lanes].astype(F32)
        for j in range(taps):
            spread[j] = jnp.broadcast_to(weights[j : j + 1, :], (8, LANES))

        def body(i, carry):
            at = pl.multiple_of(i * step, step)
            total = [None] * GROUP
            for s in range(8):
                overs = range(s, taps, 8)
                there = [
                    heights[pl.ds(at + (8 * m + s), 8), :] for m in range(GROUP + len(overs) - 1)
                ]
                for q, over in enumerate(overs):
                    weight = spread[reach - over]
                    for b in range(GROUP):
                        term = weight * there[b + q]
                        total[b] = term if total[b] is None else total[b] + term
            here = pl.ds(at, step)
            gated_grad = jnp.concatenate(total, axis=0)
            sig = jax.nn.sigmoid(gate_ref[here, lanes].astype(F32))
            grad_value = gated_grad * sig
            grad_value_ref[here, there_lanes] = grad_value.astype(BF16)
            grad_gate_ref[here, there_lanes] = (
                grad_value * value_ref[here, lanes].astype(F32) * (1.0 - sig)
            ).astype(BF16)
            return carry

        lax.fori_loop(0, rows // step, body, 0)

    strips(one, begin, begin + grad_value_ref.shape[1])


def added(refs, at=slice(None)):
    return functools.reduce(lambda a, b: a + b, [r[at, :].astype(F32) for r in refs])


def second_kernel(n, *refs):
    landed, small, outs = refs[:n], refs[n : 2 * n], refs[2 * n :]
    rows = landed[0].shape[0] // n
    more = added(small).astype(BF16)
    for k, out in enumerate(outs):
        out[0:rows, :] = added(landed, slice(k * rows, (k + 1) * rows)).astype(BF16)
        out[rows:, :] = more


def third_kernel(*refs):
    landed, (keep_ref, send_ref) = refs[:-2], refs[-2:]
    rows = keep_ref.shape[0]
    keep_ref[...] = added(landed, slice(0, rows))
    send_ref[...] = added(landed, slice(rows, None)).astype(BF16)


def fourth_kernel(keep_ref, sent_ref, came_ref, *outs):
    rows = keep_ref.shape[0]
    own = rows // len(outs)
    small = added((sent_ref, came_ref), slice(rows, None)).astype(BF16)
    for k, out in enumerate(outs):
        at = slice(k * own, (k + 1) * own)
        out[0:own, :] = added((keep_ref, came_ref), at).astype(out.dtype)
        out[own:, :] = small.astype(out.dtype)


def last_kernel(taps, *refs):
    landed, (project_ref, taps_ref, gain_ref, shift_ref) = refs[:-4], refs[-4:]
    own = project_ref.shape[0]
    total = added(landed)
    project_ref[...] = total[:own, :]
    taps_ref[...] = total[own : own + taps, :]
    gain_ref[...] = total[own + taps, :]
    shift_ref[...] = total[own + taps + 1, :]


def local(conv_value, conv_gate, conv_out, conv_taps, norm_gain, norm_shift, proj_weight, out_grad):
    rows, chans = conv_value.shape
    width = out_grad.shape[1]
    taps = conv_taps.shape[0]
    nz, n, _, cores = (lax.axis_size(a) for a in ALL)
    tail = taps + 1
    extra = -(-(taps + 2) // 8) * 8
    own = width // (nz * n * n)

    z, y, x, core = (lax.axis_index(a) for a in ALL)
    group = lax.iota(jnp.int32, nz * n * n)
    off_y, off_x = (group // n) % n ^ y, group % n ^ x

    def pair_bits(off):
        first = ((off == 1) | (off == 2)).astype(jnp.int32)
        second = (off >= 2).astype(jnp.int32)
        return jnp.where(core == 0, first, second), jnp.where(core == 0, second, first)

    (now_y, then_y), (now_x, then_x) = pair_bits(off_y), pair_bits(off_x)
    to_z = group // (n * n)
    odd = (to_z + z) % 2
    slot_z = odd * (nz // 2) + (to_z + nz - (z ^ odd)) % nz // 2
    ahead = (2 * now_y + now_x) * n + 2 * then_y + then_x
    place = (ahead * nz + slot_z) * own

    places = [
        (z, y, x, c) for z in range(nz) for y in range(n) for x in range(n) for c in range(cores)
    ]

    def index(z, y, x, c):
        return ((z * n + y) * n + x) * cores + c

    def hop(array, k, stage):
        def to(z, y, x, c):
            step = 1 if (c == 0) == (stage == 1) else 3
            return index(z, y ^ k // 2 * step, x ^ k % 2 * step, c)

        return lax.ppermute(array, ALL, [(index(*at), to(*at)) for at in places])

    def hop_z(array, k):
        return lax.ppermute(array, "sp_0", [(i, (i + k) % nz) for i in range(nz)])

    def swap_z(array):
        return lax.ppermute(array, "sp_0", [(i, i ^ 1) for i in range(nz)])

    def other_core(array):
        return lax.ppermute(array, "tp", [(0, 1), (1, 0)])

    def previous(array):
        return lax.ppermute(array, SP, [(i, i - 1) for i in range(1, nz * n * n)])

    stats, height, grads = call(
        stats_kernel,
        (
            shape((rows, LANES), F32), shape(conv_out.shape, BF16), shape(out_grad.shape, BF16),
        ),
        place, *(pltpu.with_memory_space_constraint(a, pltpu.HBM) for a in (conv_out, out_grad)),
        flops=rows * chans * 100,
        scratch=[pltpu.SemaphoreType.DMA] * 2,
        specs=[pl.BlockSpec(memory_space=pltpu.SMEM)] + [pl.BlockSpec(memory_space=pltpu.HBM)] * 2,
    )
    stats_peer = other_core(stats)
    (turned,) = call(
        turn_kernel,
        (shape((width, rows), BF16),),
        place, grads,
        flops=rows * width * chans,
        specs=[pl.BlockSpec(memory_space=pltpu.SMEM)] + vmem(1),
    )
    active, normed, deriv, inv = call(
        active_kernel,
        (
            shape((rows, chans), BF16), shape((rows, chans), F32), shape((rows, chans), F32),
            shape((rows, LANES), F32),
        ),
        height, stats, stats_peer, norm_gain, norm_shift,
        flops=rows * chans * 1000,
        scratch=[pltpu.VMEM((rows, LANES), F32)],
    )

    def project(*which):
        return call(
            functools.partial(project_kernel, which),
            (shape((width // n, chans), BF16),) * len(which),
            turned, active,
            flops=2 * rows * width * chans * len(which) // n,
        )

    blocks = {}
    blocks.update(zip((1, 2), project(1, 2)))
    (act_grad,) = call(
        matmul_kernel,
        (shape((rows, chans), F32),),
        grads, proj_weight,
        flops=2 * rows * width * chans,
    )
    lifted, sums, params = call(
        middle_kernel,
        (shape((rows, chans), F32), shape((rows, LANES), F32), shape((2, chans), F32)),
        act_grad, normed, deriv, inv, norm_gain,
        flops=rows * chans * 1000,
        scratch=[pltpu.VMEM((rows, LANES), F32)] * 2,
    )
    sums_peer = other_core(sums)
    blocks.update(zip((3, 0), project(3, 0)))
    mean, slope, head = call(
        head_kernel,
        (shape((rows, LANES), F32), shape((rows, LANES), F32), shape((tail, chans), BF16)),
        lifted, normed, inv, sums, sums_peer,
        flops=rows * chans * 10,
    )
    halo = previous(head)
    landed = [blocks[0], hop(blocks[1], 1, 1)]
    landed.append(hop(blocks[2], 2, 1))
    landed.append(hop(blocks[3], 3, 1))
    heights = (lifted, normed, mean, slope, halo)
    (small,) = call(
        taps_kernel,
        (shape((extra, chans), BF16),),
        conv_value, conv_gate, *heights, params,
        flops=taps * rows * chans * 40,
        scratch=[pltpu.VMEM((rows + tail, LANES), F32), pltpu.VMEM((rows, LANES), F32),
            pltpu.VMEM((extra, LANES), F32),
        ],
    )

    def spread_part(part, before):
        half = chans // 2
        operands = (conv_value, conv_gate, *heights, conv_taps)
        block = pl.BlockSpec((rows, half), lambda i: (0, part))
        return pl.pallas_call(
            functools.partial(spread_kernel, part * half),
            grid=(1,),
            out_shape=(shape((rows, chans), BF16),) * 2,
            in_specs=vmem(len(operands)) + [pl.BlockSpec(memory_space=pl.ANY)] * len(before),
            out_specs=(block, block),
            input_output_aliases={len(operands) + k: k for k in range(len(before))},
            scratch_shapes=[
                pltpu.VMEM((rows + tail, LANES), F32), pltpu.VMEM((taps, 8, LANES), F32),
            ],
            cost_estimate=pl.CostEstimate(
                flops=taps * rows * chans * 20, bytes_accessed=rows * chans * 10, transcendentals=0
            ),
            compiler_params=pltpu.CompilerParams(vmem_limit_bytes=8 * MIB),
            name="spread",
        )(*operands, *before)

    halves = spread_part(0, ())
    grad_value, grad_gate = spread_part(1, halves)
    smalls = [small] + [hop(small, k, 1) for k in range(1, n)]
    part = width // (n * n)
    second = call(
        functools.partial(second_kernel, n),
        (shape((part + extra, chans), BF16),) * n,
        *landed, *smalls,
        flops=width * chans * 100,
    )
    then = [second[0]] + [hop(second[k], k, 2) for k in range(1, n)]
    keep, send = call(
        third_kernel,
        (shape((part // 2, chans), F32), shape((part // 2 + extra, chans), BF16)),
        *then,
        flops=width * chans * 10,
    )
    came = swap_z(send)
    fourth = call(
        fourth_kernel,
        (shape((own + extra, chans), F32),) + (shape((own + extra, chans), BF16),) * (nz // 2 - 1),
        keep, send, came,
        flops=width * chans * 10,
    )
    fars = [fourth[0]] + [hop_z(fourth[k], 2 * k) for k in range(1, nz // 2)]
    grad_proj, grad_taps, grad_gain, grad_shift = call(
        functools.partial(last_kernel, taps),
        (shape((own, chans), F32), shape((taps, chans), F32), shape((chans,), F32), shape((chans,), F32)),
        *fars,
        flops=width * chans * 10,
    )
    return grad_value, grad_gate, grad_taps, grad_gain, grad_shift, grad_proj


def solution(mesh):
    split = Mesh(mesh.devices.reshape(8, 4, 4, mesh.shape["tp"]), ALL)
    placed = (
        P(SP, "tp"),
        P(SP, "tp"),
        P(SP, "tp"),
        P(None, "tp"),
        P("tp"),
        P("tp"),
        P(None, "tp"),
        P(SP, None),
    )
    return jax.shard_map(
        local,
        mesh=split,
        in_specs=placed,
        out_specs=(P(SP, "tp"), P(SP, "tp"), P(None, "tp"), P("tp"), P("tp"), P(SP, "tp")),
        check_vma=False,
    )
```

```python
import functools

import jax
import jax.numpy as jnp
from jax import lax
from jax.experimental import pallas as pl
from jax.experimental.pallas import tpu as pltpu
from jax.sharding import Mesh
from jax.sharding import PartitionSpec as P


SP = ("sp_0", "sp_1", "sp_2")
ALL = SP + ("tp",)
EPS = 1e-05
F32 = jnp.float32
BF16 = jnp.bfloat16
LANES = 128
MIB = 1024 * 1024


def vmem(count):
    return [pl.BlockSpec(memory_space=pltpu.VMEM)] * count


def call(kernel, outs, *args, flops, scratch=(), specs=None, limit=8):
    moved = sum(a.size * a.dtype.itemsize for a in args) + sum(
        o.size * o.dtype.itemsize for o in outs
    )
    return pl.pallas_call(
        kernel,
        out_shape=outs,
        in_specs=specs or vmem(len(args)),
        out_specs=vmem(len(outs)),
        scratch_shapes=list(scratch),
        cost_estimate=pl.CostEstimate(flops=flops, bytes_accessed=moved, transcendentals=0),
        compiler_params=pltpu.CompilerParams(vmem_limit_bytes=limit * MIB),
    )(*args)


def shape(dims, dtype):
    return jax.ShapeDtypeStruct(dims, dtype)


def left_half(rows):
    return lax.broadcasted_iota(jnp.int32, (rows, LANES), 1) < LANES // 2


def both(packed):
    left = left_half(packed.shape[0])
    turned = pltpu.roll(packed, LANES // 2, 1)
    return jnp.where(left, packed, turned), jnp.where(left, turned, packed)


def tiles(chans):
    return [slice(at, at + LANES) for at in range(0, chans, LANES)]


def stats_kernel(
    place_ref, conv_hbm, grad_hbm, stats_ref, conv_ref, grad_ref, conv_sem, grad_sem
):
    loads = [
        pltpu.make_async_copy(conv_hbm, conv_ref, conv_sem),
        pltpu.make_async_copy(grad_hbm, grad_ref, grad_sem),
    ]
    for load in loads:
        load.start()
    loads[0].wait()
    rows, chans = conv_ref.shape
    step = 128
    left = left_half(step)
    for begin in range(0, rows, step):
        at = slice(begin, begin + step)
        total = jnp.sum(
            sum(conv_ref[at, c].astype(F32) for c in tiles(chans)), axis=1, keepdims=True
        )
        mean = jnp.broadcast_to(total * (1.0 / chans), (step, LANES))
        spread = 0.0
        for c in tiles(chans):
            off = conv_ref[at, c].astype(F32) - mean
            spread = spread + off * off
        stats_ref[at, :] = jnp.where(left, total, jnp.sum(spread, axis=1, keepdims=True))
    loads[1].wait()


def turn_kernel(place_ref, grad_ref, turned_ref):
    _, width = grad_ref.shape
    piece = width // place_ref.shape[0]
    span = LANES
    each = span // piece

    def body(b, carry):
        columns = pl.ds(pl.multiple_of(b * span, span), span)
        turned = grad_ref[:, columns].T
        for p in range(each):
            to = place_ref[b * each + p]
            turned_ref[pl.ds(pl.multiple_of(to, piece), piece), :] = turned[
                p * piece : (p + 1) * piece, :
            ]
        return carry

    lax.fori_loop(0, width // span, body, 0, unroll=4)


def matmul_kernel(grad_ref, weight_ref, act_grad_ref):
    act_grad_ref[...] = jnp.dot(grad_ref[...], weight_ref[...], preferred_element_type=F32)


def active_kernel(
    conv_ref, own_ref, peer_ref, gain_ref, shift_ref,
    active_ref, normed_ref, deriv_ref, inv_ref, center_ref,
):
    rows, chans = conv_ref.shape
    wide = 128
    for begin in range(0, rows, wide):
        at = slice(begin, begin + wide)
        sum_a, dev_a = both(own_ref[at, :])
        sum_b, dev_b = both(peer_ref[at, :])
        apart = (sum_a - sum_b) * (1.0 / chans)
        variance = (dev_a + dev_b + apart * apart * (0.5 * chans)) * (0.5 / chans)
        center_ref[at, :] = (sum_a + sum_b) * (0.5 / chans)
        inv_ref[at, :] = lax.rsqrt(variance + EPS)
    step = 32

    def body(i, carry):
        at = pl.ds(pl.multiple_of(i * step, step), step)
        center, inv = center_ref[at, :], inv_ref[at, :]
        for c in tiles(chans):
            gain, shift = gain_ref[c].reshape(1, LANES), shift_ref[c].reshape(1, LANES)
            normed = (conv_ref[at, c].astype(F32) - center) * inv
            shifted = normed * gain + shift
            sig = jax.nn.sigmoid(shifted)
            active = shifted * sig
            active_ref[at, c] = active.astype(BF16)
            normed_ref[at, c] = normed
            deriv_ref[at, c] = sig + active * (1.0 - sig)
        return carry

    lax.fori_loop(0, rows // step, body, 0)


def middle_kernel(
    act_grad_ref, normed_ref, deriv_ref, inv_ref, gain_ref, lifted_ref, sums_ref, params_ref,
    total_ref, dot_ref,
):
    rows, chans = act_grad_ref.shape
    wide = 128
    step = 32

    def fold(x):
        return jnp.sum(x.reshape(step // 8, 8, LANES), axis=0)

    def body(i, carry):
        out = []
        at = pl.ds(pl.multiple_of(i * step, step), step)
        inv = inv_ref[at, :]
        total, dot = 0.0, 0.0
        for k, c in enumerate(tiles(chans)):
            normed = normed_ref[at, c]
            norm_grad = act_grad_ref[at, c] * deriv_ref[at, c]
            along = norm_grad * normed
            gain = gain_ref[c].reshape(1, LANES)
            scaled = norm_grad * gain
            lifted_ref[at, c] = scaled * inv
            total = total + scaled
            dot = dot + along * gain
            out.append(carry[2 * k] + fold(along))
            out.append(carry[2 * k + 1] + fold(norm_grad))
        total_ref[at, :] = total
        dot_ref[at, :] = dot
        return tuple(out)

    zero = jnp.zeros((8, LANES), F32)
    folded = lax.fori_loop(0, rows // step, body, (zero,) * (2 * len(tiles(chans))))
    for k, c in enumerate(tiles(chans)):
        params_ref[0:1, c] = jnp.sum(folded[2 * k], axis=0, keepdims=True)
        params_ref[1:2, c] = jnp.sum(folded[2 * k + 1], axis=0, keepdims=True)
    left = left_half(wide)
    for begin in range(0, rows, wide):
        at = slice(begin, begin + wide)
        sums_ref[at, :] = jnp.where(
            left,
            jnp.sum(total_ref[at, :], axis=1, keepdims=True),
            jnp.sum(dot_ref[at, :], axis=1, keepdims=True),
        )


def project_kernel(which, turned_ref, active_ref, *out_refs):
    rows = out_refs[0].shape[0]
    for k, out_ref in zip(which, out_refs):
        out_ref[...] = jnp.dot(
            turned_ref[k * rows : (k + 1) * rows, :], active_ref[...], preferred_element_type=F32
        ).astype(BF16)


def head_kernel(
    lifted_ref, normed_ref, inv_ref, sums_ref, sums_peer_ref, mean_ref, slope_ref, head_ref
):
    rows, chans = lifted_ref.shape
    wide = 128
    for begin in range(0, rows, wide):
        at = slice(begin, begin + wide)
        total, dot = both(sums_ref[at, :] + sums_peer_ref[at, :])
        scale = inv_ref[at, :] * (0.5 / chans)
        mean_ref[at, :] = total * scale
        slope_ref[at, :] = dot * scale
    at = slice(0, head_ref.shape[0])
    for c in tiles(chans):
        head_ref[at, c] = (
            lifted_ref[at, c] - mean_ref[at, :] - normed_ref[at, c] * slope_ref[at, :]
        ).astype(BF16)


def fill_heights(heights, lanes, lifted_ref, normed_ref, mean_ref, slope_ref, halo_ref):
    rows = lifted_ref.shape[0]
    tail = halo_ref.shape[0]
    heights[0:rows, :] = (
        lifted_ref[:, lanes] - mean_ref[...] - normed_ref[:, lanes] * slope_ref[...]
    )
    heights[rows : rows + tail, :] = halo_ref[:, lanes].astype(F32)


def strips(body, begin, end):
    def step(i, carry):
        body(i * LANES)
        return carry

    lax.fori_loop(begin // LANES, end // LANES, step, 0)


def lanes_at(at):
    return pl.ds(pl.multiple_of(at, LANES), LANES)


GROUP = 8


def taps_kernel(
    value_ref, gate_ref, lifted_ref, normed_ref, mean_ref, slope_ref, halo_ref, params_ref,
    out_ref, heights, gated, rows_ref,
):
    rows, chans = value_ref.shape
    taps = halo_ref.shape[0] - 1
    reach = taps - 1
    step = 8 * GROUP

    def one(lanes):
        fill_heights(heights, lanes, lifted_ref, normed_ref, mean_ref, slope_ref, halo_ref)
        sig = jax.nn.sigmoid(gate_ref[:, lanes].astype(F32))
        gated[...] = (value_ref[:, lanes].astype(F32) * sig).astype(BF16).astype(F32)

        def body(i, sums):
            at = pl.multiple_of(i * step, step)
            held = [gated[pl.ds(at + 8 * b, 8), :] for b in range(GROUP)]
            out = list(sums)
            for s in range(8):
                overs = range(s, taps, 8)
                there = [
                    heights[pl.ds(at + (8 * m + s), 8), :] for m in range(GROUP + len(overs) - 1)
                ]
                for q, over in enumerate(overs):
                    j = reach - over
                    products = [held[b] * there[b + q] for b in range(GROUP)]
                    while len(products) > 1:
                        products = [a + b for a, b in zip(products[::2], products[1::2])]
                    out[j] = out[j] + products[0]
            return tuple(out)

        zero = jnp.zeros((8, LANES), F32)
        sums = lax.fori_loop(0, rows // step, body, (zero,) * taps)
        for j in range(taps):
            rows_ref[j : j + 1, :] = jnp.sum(sums[j], axis=0, keepdims=True)
        rows_ref[taps : taps + 2, :] = params_ref[:, lanes]
        rows_ref[taps + 2 :, :] = jnp.zeros((rows_ref.shape[0] - taps - 2, LANES), F32)
        out_ref[:, lanes] = rows_ref[...].astype(BF16)

    strips(lambda at: one(lanes_at(at)), 0, chans)


def spread_kernel(
    begin, value_ref, gate_ref, lifted_ref, normed_ref, mean_ref, slope_ref, halo_ref, taps_ref, *refs
):
    grad_value_ref, grad_gate_ref, heights, spread = refs[-4:]
    rows = value_ref.shape[0]
    taps = taps_ref.shape[0]
    reach = taps - 1
    step = 8 * GROUP

    def one(at_lane):
        lanes, there_lanes = lanes_at(at_lane), lanes_at(at_lane - begin)
        fill_heights(heights, lanes, lifted_ref, normed_ref, mean_ref, slope_ref, halo_ref)
        weights = taps_ref[:, lanes].astype(F32)
        for j in range(taps):
            spread[j] = jnp.broadcast_to(weights[j : j + 1, :], (8, LANES))

        def body(i, carry):
            at = pl.multiple_of(i * step, step)
            total = [None] * GROUP
            for s in range(8):
                overs = range(s, taps, 8)
                there = [
                    heights[pl.ds(at + (8 * m + s), 8), :] for m in range(GROUP + len(overs) - 1)
                ]
                for q, over in enumerate(overs):
                    weight = spread[reach - over]
                    for b in range(GROUP):
                        term = weight * there[b + q]
                        total[b] = term if total[b] is None else total[b] + term
            here = pl.ds(at, step)
            gated_grad = jnp.concatenate(total, axis=0)
            sig = jax.nn.sigmoid(gate_ref[here, lanes].astype(F32))
            grad_value = gated_grad * sig
            grad_value_ref[here, there_lanes] = grad_value.astype(BF16)
            grad_gate_ref[here, there_lanes] = (
                grad_value * value_ref[here, lanes].astype(F32) * (1.0 - sig)
            ).astype(BF16)
            return carry

        lax.fori_loop(0, rows // step, body, 0)

    strips(one, begin, begin + grad_value_ref.shape[1])


def added(refs, at=slice(None)):
    return functools.reduce(lambda a, b: a + b, [r[at, :].astype(F32) for r in refs])


def second_kernel(n, *refs):
    landed, small, outs = refs[:n], refs[n : 2 * n], refs[2 * n :]
    rows = landed[0].shape[0] // n
    more = added(small).astype(BF16)
    for k, out in enumerate(outs):
        out[0:rows, :] = added(landed, slice(k * rows, (k + 1) * rows)).astype(BF16)
        out[rows:, :] = more


def third_kernel(*refs):
    landed, (keep_ref, send_ref) = refs[:-2], refs[-2:]
    rows = keep_ref.shape[0]
    keep_ref[...] = added(landed, slice(0, rows))
    send_ref[...] = added(landed, slice(rows, None)).astype(BF16)


def fourth_kernel(keep_ref, sent_ref, came_ref, *outs):
    rows = keep_ref.shape[0]
    own = rows // len(outs)
    small = added((sent_ref, came_ref), slice(rows, None)).astype(BF16)
    for k, out in enumerate(outs):
        at = slice(k * own, (k + 1) * own)
        out[0:own, :] = added((keep_ref, came_ref), at).astype(out.dtype)
        out[own:, :] = small.astype(out.dtype)


def last_kernel(taps, *refs):
    landed, (project_ref, taps_ref, gain_ref, shift_ref) = refs[:-4], refs[-4:]
    own = project_ref.shape[0]
    total = added(landed)
    project_ref[...] = total[:own, :]
    taps_ref[...] = total[own : own + taps, :]
    gain_ref[...] = total[own + taps, :]
    shift_ref[...] = total[own + taps + 1, :]


def local(conv_value, conv_gate, conv_out, conv_taps, norm_gain, norm_shift, proj_weight, out_grad):
    rows, chans = conv_value.shape
    width = out_grad.shape[1]
    taps = conv_taps.shape[0]
    nz, n, _, cores = (lax.axis_size(a) for a in ALL)
    tail = taps + 1
    extra = -(-(taps + 2) // 8) * 8
    own = width // (nz * n * n)

    z, y, x, core = (lax.axis_index(a) for a in ALL)
    group = lax.iota(jnp.int32, nz * n * n)
    off_y, off_x = (group // n) % n ^ y, group % n ^ x

    def pair_bits(off):
        first = ((off == 1) | (off == 2)).astype(jnp.int32)
        second = (off >= 2).astype(jnp.int32)
        return jnp.where(core == 0, first, second), jnp.where(core == 0, second, first)

    (now_y, then_y), (now_x, then_x) = pair_bits(off_y), pair_bits(off_x)
    to_z = group // (n * n)
    odd = (to_z + z) % 2
    slot_z = odd * (nz // 2) + (to_z + nz - (z ^ odd)) % nz // 2
    ahead = (2 * now_y + now_x) * n + 2 * then_y + then_x
    place = (ahead * nz + slot_z) * own

    places = [
        (z, y, x, c) for z in range(nz) for y in range(n) for x in range(n) for c in range(cores)
    ]

    def index(z, y, x, c):
        return ((z * n + y) * n + x) * cores + c

    def hop(array, k, stage):
        def to(z, y, x, c):
            step = 1 if (c == 0) == (stage == 1) else 3
            return index(z, y ^ k // 2 * step, x ^ k % 2 * step, c)

        return lax.ppermute(array, ALL, [(index(*at), to(*at)) for at in places])

    def hop_z(array, k):
        return lax.ppermute(array, "sp_0", [(i, (i + k) % nz) for i in range(nz)])

    def swap_z(array):
        return lax.ppermute(array, "sp_0", [(i, i ^ 1) for i in range(nz)])

    def other_core(array):
        return lax.ppermute(array, "tp", [(0, 1), (1, 0)])

    def previous(array):
        return lax.ppermute(array, SP, [(i, i - 1) for i in range(1, nz * n * n)])

    stats, height, grads = call(
        stats_kernel,
        (
            shape((rows, LANES), F32), shape(conv_out.shape, BF16), shape(out_grad.shape, BF16),
        ),
        place, *(pltpu.with_memory_space_constraint(a, pltpu.HBM) for a in (conv_out, out_grad)),
        flops=rows * chans * 100,
        scratch=[pltpu.SemaphoreType.DMA] * 2,
        specs=[pl.BlockSpec(memory_space=pltpu.SMEM)] + [pl.BlockSpec(memory_space=pltpu.HBM)] * 2,
    )
    stats_peer = other_core(stats)
    (turned,) = call(
        turn_kernel,
        (shape((width, rows), BF16),),
        place, grads,
        flops=rows * width * chans,
        specs=[pl.BlockSpec(memory_space=pltpu.SMEM)] + vmem(1),
    )
    active, normed, deriv, inv = call(
        active_kernel,
        (
            shape((rows, chans), BF16), shape((rows, chans), F32), shape((rows, chans), F32),
            shape((rows, LANES), F32),
        ),
        height, stats, stats_peer, norm_gain, norm_shift,
        flops=rows * chans * 1000,
        scratch=[pltpu.VMEM((rows, LANES), F32)],
    )

    def project(*which):
        return call(
            functools.partial(project_kernel, which),
            (shape((width // n, chans), BF16),) * len(which),
            turned, active,
            flops=2 * rows * width * chans * len(which) // n,
        )

    blocks = {}
    blocks.update(zip((1, 2), project(1, 2)))
    (act_grad,) = call(
        matmul_kernel,
        (shape((rows, chans), F32),),
        grads, proj_weight,
        flops=2 * rows * width * chans,
    )
    lifted, sums, params = call(
        middle_kernel,
        (shape((rows, chans), F32), shape((rows, LANES), F32), shape((2, chans), F32)),
        act_grad, normed, deriv, inv, norm_gain,
        flops=rows * chans * 1000,
        scratch=[pltpu.VMEM((rows, LANES), F32)] * 2,
    )
    sums_peer = other_core(sums)
    blocks.update(zip((3, 0), project(3, 0)))
    mean, slope, head = call(
        head_kernel,
        (shape((rows, LANES), F32), shape((rows, LANES), F32), shape((tail, chans), BF16)),
        lifted, normed, inv, sums, sums_peer,
        flops=rows * chans * 10,
    )
    halo = previous(head)
    landed = [blocks[0], hop(blocks[1], 1, 1)]
    landed.append(hop(blocks[2], 2, 1))
    landed.append(hop(blocks[3], 3, 1))
    heights = (lifted, normed, mean, slope, halo)
    (small,) = call(
        taps_kernel,
        (shape((extra, chans), BF16),),
        conv_value, conv_gate, *heights, params,
        flops=taps * rows * chans * 40,
        scratch=[pltpu.VMEM((rows + tail, LANES), F32), pltpu.VMEM((rows, LANES), F32),
            pltpu.VMEM((extra, LANES), F32),
        ],
    )

    def spread_part(part, before):
        half = chans // 2
        operands = (conv_value, conv_gate, *heights, conv_taps)
        block = pl.BlockSpec((rows, half), lambda i: (0, part))
        return pl.pallas_call(
            functools.partial(spread_kernel, part * half),
            grid=(1,),
            out_shape=(shape((rows, chans), BF16),) * 2,
            in_specs=vmem(len(operands)) + [pl.BlockSpec(memory_space=pl.ANY)] * len(before),
            out_specs=(block, block),
            input_output_aliases={len(operands) + k: k for k in range(len(before))},
            scratch_shapes=[
                pltpu.VMEM((rows + tail, LANES), F32), pltpu.VMEM((taps, 8, LANES), F32),
            ],
            cost_estimate=pl.CostEstimate(
                flops=taps * rows * chans * 20, bytes_accessed=rows * chans * 10, transcendentals=0
            ),
            compiler_params=pltpu.CompilerParams(vmem_limit_bytes=8 * MIB),
            name="spread",
        )(*operands, *before)

    halves = spread_part(0, ())
    grad_value, grad_gate = spread_part(1, halves)
    smalls = [small] + [hop(small, k, 1) for k in range(1, n)]
    part = width // (n * n)
    second = call(
        functools.partial(second_kernel, n),
        (shape((part + extra, chans), BF16),) * n,
        *landed, *smalls,
        flops=width * chans * 100,
    )
    then_long = hop(second[3], 3, 2)
    then = [second[0], hop(second[1], 1, 2), hop(second[2], 2, 2), then_long]
    keep, send = call(
        third_kernel,
        (shape((part // 2, chans), F32), shape((part // 2 + extra, chans), BF16)),
        *then,
        flops=width * chans * 10,
    )
    came = swap_z(send)
    fourth = call(
        fourth_kernel,
        (shape((own + extra, chans), F32),) + (shape((own + extra, chans), BF16),) * (nz // 2 - 1),
        keep, send, came,
        flops=width * chans * 10,
    )
    long = hop_z(fourth[2], 4)
    fars = [fourth[0], hop_z(fourth[1], 2), long, hop_z(fourth[3], 6)]
    grad_proj, grad_taps, grad_gain, grad_shift = call(
        functools.partial(last_kernel, taps),
        (shape((own, chans), F32), shape((taps, chans), F32), shape((chans,), F32), shape((chans,), F32)),
        *fars,
        flops=width * chans * 10,
    )
    return grad_value, grad_gate, grad_taps, grad_gain, grad_shift, grad_proj


def solution(mesh):
    split = Mesh(mesh.devices.reshape(8, 4, 4, mesh.shape["tp"]), ALL)
    placed = (
        P(SP, "tp"),
        P(SP, "tp"),
        P(SP, "tp"),
        P(None, "tp"),
        P("tp"),
        P("tp"),
        P(None, "tp"),
        P(SP, None),
    )
    return jax.shard_map(
        local,
        mesh=split,
        in_specs=placed,
        out_specs=(P(SP, "tp"), P(SP, "tp"), P(None, "tp"), P("tp"), P("tp"), P(SP, "tp")),
        check_vma=False,
    )
```
